32 devices in a mesh: sp: 4 (over z), fs: 4 (over y, core), tp: 2 (over x).
Axes of the slice: x: 2, y: 2, z: 4, core: 2. Of those that a mesh axis runs over, the one named last changes fastest.
Arguments:
- tokens: bfloat16 [4096, 2048], P(('fs', 'sp', 'tp')), parts along dimension 0, may hold values from -6 to 6
- norm_gain: bfloat16 [2048], replicated, may hold values from 0.099609375 to 1.8984375
- w_pool_in: bfloat16 [2048, 1024], P('sp', 'tp'), may hold values from -0.125 to 0.125
- w_query: bfloat16 [2048, 1024], P('sp', 'tp'), may hold values from -0.125 to 0.125
- w_key: bfloat16 [2048, 1024], P('sp', 'tp'), may hold values from -0.125 to 0.125
- w_value: bfloat16 [2048, 1024], P('sp', 'tp'), may hold values from -0.125 to 0.125
- w_gate: bfloat16 [2048, 1024], P('sp', 'tp'), may hold values from -0.125 to 0.125
- w_beta: bfloat16 [2048, 8], replicated, may hold values from -0.125 to 0.125
- w_decay: bfloat16 [2048, 8], replicated, may hold values from -0.5 to 0.5
- conv_weight: float32 [3, 4, 1024], P(None, None, 'tp'), may hold values from -3 to 3
- a_log: float32 [8], P('tp'), may hold values from -20 to -1.7, as said below
- decay_extra: float32 [4096, 8], P(('fs', 'sp'), 'tp'), parts along dimension 0, may hold values from -1.4 to 0
- w_mix: bfloat16 [8, 128, 128], P('tp'), may hold values from -0.5 to 0.5
- pool_scale: float32 [1024], P('tp'), may hold values from 0.1 to 1.9
- delta_gain: float32 [128], replicated, may hold values from 0.1 to 1.9
- w_out_pool: bfloat16 [1024, 2048], P('tp', 'sp'), may hold values from -0.125 to 0.125
- w_out_delta: bfloat16 [1024, 2048], P('tp', 'sp'), may hold values from -0.125 to 0.125
Outputs:
- mixed: bfloat16 [4096, 2048], P(('fs', 'sp', 'tp')), parts along dimension 0
The draws below stay inside these ranges and needn't reach their ends.
There are 4 independent parts, one for each index of `fs`. The reference program is written for one: setup_inputs(seed, part) draws one part's arguments, and reference() takes and returns one part's arrays. A program takes and returns all parts, laid end to end along the dimension named above; an argument that names none is the same for every part. Nothing has to cross between parts.
Inputs may be any that keep to these rules, and one draw needn't show every extreme that they name: `a_log`: logarithm of each head's base decay rate.
All inputs are finite; a program needn't handle non-finite values.
Results may differ from the reference program's by a relative error of at most 0.018.
Values may be sent and summed in bfloat16 or wider, within the bound.
A program may use at most 64 MiB of HBM per device.

```python
import jax
import jax.numpy as jnp
from jax import lax

D = 2048
POOL_GROUPS = 8
GROUP_DIM = 128
DN_HEADS = 8
HEAD_DIM = 128
CONV = 4
BLOCK = 64
SP_TOK = 256
POOL_WIDTH = 1024
DN_WIDTH = 1024
SEQ = 1024
N_TP = 2


def draw_a_log(key, part):
    chooser, slow_key, fast_key = jax.random.split(jax.random.fold_in(key, 11), 3)
    fast_share = 0.5
    fast = jax.random.uniform(chooser, (DN_HEADS,), jnp.float32) < fast_share
    slow_rate = jnp.exp(jax.random.uniform(slow_key, (DN_HEADS,), jnp.float32, jnp.log(0.05), jnp.log(0.2))) / SEQ
    fast_rate = jax.random.uniform(fast_key, (DN_HEADS,), jnp.float32, 1.0 / 16.0, 1.0 / 6.0)
    return jnp.log(jnp.where(fast, fast_rate, slow_rate)).astype(jnp.float32)


def draw_decay_extra(key, part):
    rate_key, position_seed, depth_key = jax.random.split(jax.random.fold_in(key, 23), 3)
    rates = jnp.exp(jax.random.uniform(rate_key, (SEQ // SP_TOK, DN_HEADS), jnp.float32, jnp.log(0.1), jnp.log(0.6))) / SEQ
    starting_shift = -jnp.repeat(rates, SP_TOK, axis=0)
    places = jax.random.randint(position_seed, (2, DN_HEADS), 0, SEQ)
    layer_ordinal = jax.random.uniform(depth_key, (2, DN_HEADS), jnp.float32, 0.22, 0.69)
    positions = jnp.arange(SEQ, dtype=jnp.int32)
    agreeing_tally = (positions[:, None, None] == places[None, :, :]).astype(jnp.float32)
    window_bundles = -jnp.sum(agreeing_tally * layer_ordinal[None, :, :], axis=1)
    return (starting_shift + window_bundles).astype(jnp.float32)


def shard_levels(own_key, shape, shards, smallest, high):
    loudness = 1.0
    for position, parts in shards:
        heights = jax.random.uniform(jax.random.fold_in(jax.random.fold_in(own_key, 6), position), (parts,), jnp.float32, smallest / len(shards), high / len(shards))
        loudness = loudness * jnp.repeat(jnp.exp(heights), shape[position] // parts).reshape((-1,) + (1,) * (len(shape) - 1 - position))
    return loudness


def centred(stream_key, shape, scale, most, shards=(), kind=jnp.bfloat16):
    values = scale * jax.random.normal(stream_key, shape, jnp.float32)
    if shards:
        values = values * shard_levels(stream_key, shape, shards, -0.22, 0.18)
    return jnp.clip(values, -most, most).astype(kind)


def setup_inputs(seed: int = 0, part: int = 0) -> dict:
    seeds = jax.random.split(jax.random.key(seed), 18)
    part_keys = jax.random.split(jax.random.fold_in(seeds[17], part), 18)
    return {
        "tokens": centred(part_keys[0], (SEQ, D), 1.0, 6.0, ((0, 8),)),
        "norm_gain": jnp.clip(1.0 + 0.18 * jax.random.normal(seeds[1], (D,), jnp.float32), 0.099609375, 1.8984375).astype(jnp.bfloat16),
        "w_pool_in": centred(seeds[2], (D, POOL_WIDTH), D ** -0.5, 0.125, ((0, 4), (1, 2))),
        "w_query": centred(seeds[3], (D, DN_WIDTH), D ** -0.5, 0.125, ((0, 4), (1, 2))),
        "w_key": centred(seeds[4], (D, DN_WIDTH), D ** -0.5, 0.125, ((0, 4), (1, 2))),
        "w_value": centred(seeds[5], (D, DN_WIDTH), D ** -0.5, 0.125, ((0, 4), (1, 2))),
        "w_gate": centred(seeds[6], (D, DN_WIDTH), D ** -0.5, 0.125, ((0, 4), (1, 2))),
        "w_beta": centred(seeds[7], (D, DN_HEADS), D ** -0.5, 0.125),
        "w_decay": centred(seeds[8], (D, DN_HEADS), (D // 16) ** -0.5, 0.5),
        "conv_weight": centred(seeds[9], (3, CONV, DN_WIDTH), CONV ** -0.5, 3.0, ((2, 2),), jnp.float32),
        "a_log": draw_a_log(jax.random.fold_in(seeds[17], 71), part),
        "decay_extra": draw_decay_extra(jax.random.fold_in(jax.random.fold_in(seeds[17], part), 71), part),
        "w_mix": centred(seeds[12], (POOL_GROUPS, GROUP_DIM, GROUP_DIM), GROUP_DIM ** -0.5, 0.5, ((0, 2),)),
        "pool_scale": jnp.clip(1.0 + 0.18 * jax.random.normal(seeds[13], (POOL_WIDTH,), jnp.float32), 0.1, 1.9),
        "delta_gain": jnp.clip(1.0 + 0.18 * jax.random.normal(seeds[14], (HEAD_DIM,), jnp.float32), 0.1, 1.9),
        "w_out_pool": centred(seeds[15], (POOL_WIDTH, D), (POOL_WIDTH + DN_WIDTH) ** -0.5, 0.125, ((0, 2), (1, 4))),
        "w_out_delta": centred(seeds[16], (DN_WIDTH, D), (POOL_WIDTH + DN_WIDTH) ** -0.5, 0.125, ((0, 2), (1, 4))),
    }


eps = 1e-06
windows = (2, 4, 8, 16)
highest = lax.Precision.HIGHEST

def rms_rows(values, gain):
    floats = values.astype(jnp.float32)
    scale = lax.rsqrt(lax.optimization_barrier(jnp.mean(floats * floats, axis=-1, keepdims=True)) + eps)
    return (floats * scale * gain.astype(jnp.float32)).astype(jnp.bfloat16)

def unit_rows(values):
    return values * lax.rsqrt(lax.optimization_barrier(jnp.sum(values * values, axis=-1, keepdims=True)) + eps)

def block_terms(query, keys, values, log_gate, strength, block):
    heads, length, width = keys.shape
    count = length // block

    def split(tensor):
        return tensor.reshape(heads, count, block, tensor.shape[-1])
    query_part, key_part, value_part = (split(query), split(keys), split(values))
    gate_cum = jnp.cumsum(log_gate.reshape(heads, count, block), axis=-1)
    beta_part = strength.reshape(heads, count, block)[..., None]
    lower_mask = jnp.tril(jnp.ones((block, block), dtype=bool))
    strict_mask = jnp.tril(jnp.ones((block, block), dtype=bool), k=-1)
    gaps = gate_cum[..., :, None] - gate_cum[..., None, :]
    decay_tab = jnp.where(lower_mask, jnp.exp(jnp.where(lower_mask, gaps, 0.0)), 0.0)
    key_scaled_beta = key_part * beta_part
    value_beta = value_part * beta_part
    corr_lower = jnp.where(strict_mask, jnp.einsum('hnid,hnjd->hnij', key_scaled_beta, key_part, precision=highest) * decay_tab, 0.0)
    identity = jnp.eye(block, dtype=jnp.float32)
    inverse = lax.linalg.triangular_solve(identity + corr_lower, jnp.broadcast_to(identity, corr_lower.shape), left_side=True, lower=True)
    fixed_values = jnp.einsum('hnij,hnjd->hnid', inverse, value_beta, precision=highest)
    key_weights = jnp.einsum('hnij,hnjd->hnid', inverse, key_scaled_beta * jnp.exp(gate_cum)[..., None], precision=highest)
    scores = jnp.where(lower_mask, jnp.einsum('hnid,hnjd->hnij', query_part, key_part, precision=highest) * decay_tab, 0.0)
    key_decayed = key_part * jnp.exp(gate_cum[..., -1:] - gate_cum)[..., None]
    query_gated = query_part * jnp.exp(gate_cum)[..., None]
    terms = (query_gated, key_decayed, fixed_values, key_weights, scores, gate_cum[..., -1])
    return tuple((jnp.moveaxis(tensor, 1, 0) for tensor in terms))

def carry_step(state, inputs):
    query_gated, key_decayed, fixed_values, key_weights, scores, last_gate = inputs
    fresh = fixed_values - jnp.einsum('hcd,hde->hce', key_weights, state, precision=highest)
    output = jnp.einsum('hcd,hde->hce', query_gated, state, precision=highest) + jnp.einsum('hij,hje->hie', scores, fresh, precision=highest)
    state = state * jnp.exp(last_gate)[:, None, None] + jnp.einsum('hcd,hce->hde', key_decayed, fresh, precision=highest)
    return (state, output)

def reference(tokens, norm_gain, w_pool_in, w_query, w_key, w_value, w_gate, w_beta, w_decay, conv_weight, a_log, decay_extra, w_mix, pool_scale, delta_gain, w_out_pool, w_out_delta):
    norm_result = rms_rows(tokens, norm_gain)

    def project(weight):
        return jnp.dot(norm_result.astype(jnp.float32), weight.astype(jnp.float32), preferred_element_type=jnp.float32).astype(jnp.bfloat16)
    pool_in = project(w_pool_in)
    query_raw = project(w_query)
    key_raw = project(w_key)
    value_raw = project(w_value)
    gate_raw = project(w_gate)
    beta_pre = jnp.dot(norm_result.astype(jnp.float32), w_beta.astype(jnp.float32), preferred_element_type=jnp.float32)
    forget_logits = jnp.dot(norm_result.astype(jnp.float32), w_decay.astype(jnp.float32), preferred_element_type=jnp.float32)
    source_rows = pool_in.astype(jnp.float32)
    running = jnp.concatenate([jnp.zeros((1, POOL_WIDTH), jnp.float32), jnp.cumsum(source_rows, axis=0)], axis=0)
    group = (jnp.arange(POOL_WIDTH) // GROUP_DIM).astype(jnp.int32)
    span = (2 ** (1 + group % 4)).astype(jnp.int32)
    window_sum = jnp.zeros((SEQ, POOL_WIDTH), jnp.float32)
    for width in windows:
        lagged = jnp.concatenate([jnp.zeros((width - 1, POOL_WIDTH), jnp.float32), running[:SEQ - width + 1]], axis=0)
        window_sum = window_sum + jnp.where(span[None, :] == width, running[1:] - lagged, 0.0)
    positions = jnp.arange(SEQ).astype(jnp.int32)
    counts = jnp.minimum(positions[:, None] + 1, span[None, :]).astype(jnp.float32)
    pooled = (window_sum / counts - source_rows).astype(jnp.bfloat16)
    mixed_pool = jnp.einsum('sgc,gcd->sgd', pooled.reshape(SEQ, POOL_GROUPS, GROUP_DIM).astype(jnp.float32), w_mix.astype(jnp.float32), precision=highest)
    pool_out = (mixed_pool.reshape(SEQ, POOL_WIDTH) * pool_scale).astype(jnp.bfloat16)
    stacked = jnp.concatenate([query_raw, key_raw, value_raw], axis=1).astype(jnp.float32)
    kernel = jnp.transpose(conv_weight, (1, 0, 2)).reshape(CONV, 3 * DN_WIDTH)
    padded = jnp.concatenate([jnp.zeros((CONV - 1, 3 * DN_WIDTH), jnp.float32), stacked], axis=0)
    conv = jnp.zeros((SEQ, 3 * DN_WIDTH), jnp.float32)
    for tap in range(CONV):
        conv = conv + padded[tap:tap + SEQ] * kernel[tap]
    after_silu = jax.nn.silu(conv)

    def heads_first(tensor):
        return jnp.transpose(tensor.reshape(SEQ, DN_HEADS, HEAD_DIM), (1, 0, 2))
    query = unit_rows(heads_first(after_silu[:, :DN_WIDTH])) * HEAD_DIM ** (-0.5)
    keys = unit_rows(heads_first(after_silu[:, DN_WIDTH:2 * DN_WIDTH]))
    values = heads_first(after_silu[:, 2 * DN_WIDTH:])
    strength = jax.nn.sigmoid(beta_pre).T
    log_gate = (-jnp.exp(a_log)[None, :] * jax.nn.softplus(forget_logits) + decay_extra).T
    terms = block_terms(query, keys, values, log_gate, strength, BLOCK)
    _, outputs = lax.scan(carry_step, jnp.zeros((DN_HEADS, HEAD_DIM, HEAD_DIM), jnp.float32), terms)
    attended = jnp.transpose(outputs, (1, 0, 2, 3)).reshape(DN_HEADS, SEQ, HEAD_DIM)
    normal_out = attended * lax.rsqrt(lax.optimization_barrier(jnp.mean(attended * attended, axis=-1, keepdims=True)) + eps) * delta_gain
    gated = normal_out * jax.nn.silu(heads_first(gate_raw.astype(jnp.float32)))
    delta_out = jnp.transpose(gated, (1, 0, 2)).reshape(SEQ, DN_WIDTH).astype(jnp.bfloat16)
    pool_cols = POOL_WIDTH // N_TP
    delta_cols = DN_WIDTH // N_TP
    total = jnp.zeros((SEQ, D), jnp.float32)
    for lane in range(N_TP):
        value_partial_rows = jnp.dot(pool_out[:, lane * pool_cols:(lane + 1) * pool_cols].astype(jnp.float32), w_out_pool[lane * pool_cols:(lane + 1) * pool_cols].astype(jnp.float32), preferred_element_type=jnp.float32)
        value_partial_rows = value_partial_rows + jnp.dot(delta_out[:, lane * delta_cols:(lane + 1) * delta_cols].astype(jnp.float32), w_out_delta[lane * delta_cols:(lane + 1) * delta_cols].astype(jnp.float32), preferred_element_type=jnp.float32)
        total = total + lax.optimization_barrier(value_partial_rows.astype(jnp.bfloat16)).astype(jnp.float32)
    return total.astype(jnp.bfloat16)
```

```python
import functools

import jax
import jax.numpy as jnp
from jax import lax
from jax.experimental import pallas as pl
from jax.experimental.pallas import tpu as pltpu
from jax.sharding import PartitionSpec as P

BLOCK = 64
PAIR = 2 * BLOCK

eps = 1e-06
halo = 16
MESH = pl.DeviceIdType.MESH
highest = lax.Precision.HIGHEST
f32 = jnp.float32
bf16 = jnp.bfloat16
KEY, QUERY, VALUE, POOL, GATE, OUT_POOL, OUT_DELTA = range(7)
AHEAD = 2
LAG = 2
UNROLL = 32


def mm(a, b, dims=((1,), (0,)), precision=highest):
    return lax.dot_general(a, b, (dims, ((), ())), precision=precision, preferred_element_type=f32)


def rms_rows(values, gain):
    floats = values.astype(f32)
    scale = lax.rsqrt(jnp.mean(floats * floats, axis=-1, keepdims=True) + eps)
    return (floats * scale * gain.astype(f32)).astype(bf16)


def unit_rows(values):
    return values * lax.rsqrt(jnp.sum(values * values, axis=-1, keepdims=True) + eps)


def silu(x):
    return x * jax.nn.sigmoid(x)


def share_bits(n_fs):
    if n_fs & (n_fs - 1):
        return []
    return [n_fs >> (k + 1) for k in range(n_fs.bit_length() - 1)]


def both(a, b):
    if isinstance(a, bool):
        return b if a else False
    if isinstance(b, bool):
        return a if b else False
    return jnp.logical_and(a, b)


def when(cond, act):
    if isinstance(cond, bool):
        if cond:
            act()
    else:
        pl.when(cond)(act)


class Gather:
    def __init__(self, n_sp, n_fs, wbuf, z_s, z_f, z_r, f_s, f_r, last_r):
        self.n_sp, self.bits = n_sp, share_bits(n_fs)
        self.wbuf, self.z_s, self.z_f, self.z_r, self.f_s, self.f_r, self.last_r = wbuf, z_s, z_f, z_r, f_s, f_r, last_r
        self.sp, self.fs = lax.axis_index("sp"), lax.axis_index("fs")
        self.count = wbuf.shape[0]
        self.span = n_sp - 1
        self.pieces = 2 ** len(self.bits)
        self.mine = self.fs if self.bits else 0 * self.fs
        self.depth = wbuf.shape[2] // self.pieces

    def partner(self, bit):
        return self.fs + bit * (1 - 2 * (self.fs // bit % 2))

    def mask_of(self, m, index):
        for i, bit in enumerate(self.bits):
            if m >> i & 1:
                index = index + bit * (1 - 2 * (index // bit % 2))
        return index

    def piece(self, w, src, index):
        return self.wbuf.at[w, src, pl.ds(pl.multiple_of(index * self.depth, self.depth), self.depth)]

    def z_copy(self, w, src, way, own):
        ref = self.piece(w, src, self.mine)
        to = lax.rem(self.sp + way + self.n_sp, self.n_sp)
        sent = self.z_s.at[w, (way + 1) // 2] if own else self.z_f.at[w]
        return pltpu.make_async_remote_copy(
            src_ref=ref, dst_ref=ref, send_sem=sent, recv_sem=self.z_r.at[w, src],
            device_id={"sp": to}, device_id_type=MESH)

    def f_copy(self, w, src, k, m):
        ref = self.piece(w, src, self.mask_of(m, self.mine))
        inner = k < len(self.bits) - 1
        return pltpu.make_async_remote_copy(
            src_ref=ref, dst_ref=ref, send_sem=self.f_s.at[w],
            recv_sem=self.f_r.at[w, src, 2 ** k - 1 + m] if inner else self.last_r.at[w, src],
            device_id={"fs": self.partner(self.bits[k])}, device_id_type=MESH)

    def can_send(self, way):
        return self.sp < self.n_sp - 1 if way == 1 else self.sp > 0

    def send(self, w):
        for way in (1, -1):
            @pl.when(self.can_send(way))
            def _():
                self.z_copy(w, self.sp, way, True).start()

    def each(self, t, act):
        for way in (1, -1):
            src = self.sp - way * t
            @pl.when(src >= 0 if way == 1 else src < self.n_sp)
            def _():
                act(src, way)

    def arrive_z(self, w, src, way):
        self.z_copy(w, src, way, False).wait_recv()

        @pl.when(self.can_send(way))
        def _():
            self.z_copy(w, src, way, False).start()
        for k in range(len(self.bits)):
            self.f_copy(w, src, k, 0).start()

    def arrive_f(self, w, t, k):
        def act(src, way):
            for m in range(2 ** k):
                self.f_copy(w, src, k, m).wait_recv()
                for later in range(k + 1, len(self.bits)):
                    self.f_copy(w, src, later, m | 1 << k).start()
        self.each(t, act)

    def steps(self):
        return self.count * self.span

    def step(self, i):
        w, t = i // self.span, i % self.span + 1
        when(i < self.steps(), lambda: self.each(t, lambda src, way: self.arrive_z(w, src, way)))
        when(both(t == 1, w + AHEAD < self.count), lambda: self.send(w + AHEAD))
        for k in range(len(self.bits) - 1):
            j = i - LAG * (k + 1)
            when(both(j >= 0, j < self.steps()), lambda: self.arrive_f(j // self.span, j % self.span + 1, k))

    def end(self):
        return self.steps() + LAG * max(0, len(self.bits) - 1)

    def ready(self, w, t):
        if self.bits:
            def act(src, way):
                ref = self.wbuf.at[w, src, pl.ds(0, self.wbuf.shape[2] // 2)]
                pltpu.make_async_copy(ref, ref, self.last_r.at[w, src]).wait()
            self.each(t, act)

    def finish(self, w):
        self.loop(1, self.n_sp, lambda t: self.ready(w, t))

    def drain(self, w):
        for way in (1, -1):
            @pl.when(self.can_send(way))
            def _():
                self.z_copy(w, self.sp, way, True).wait_send()
        if self.n_sp > 2:
            @pl.when(jnp.logical_and(self.can_send(1), self.can_send(-1)))
            def _():
                ref = self.wbuf.at[w, pl.ds(0, self.span), pl.ds(0, self.depth)]
                pltpu.make_async_copy(ref, ref, self.z_f.at[w]).wait()
        if self.bits:
            ref = self.wbuf.at[w, pl.ds(0, self.span), pl.ds(0, (self.pieces - 1) * self.depth)]
            pltpu.make_async_copy(ref, ref, self.f_s.at[w]).wait()

    def loop(self, a, b, act):
        if self.steps() <= UNROLL:
            for i in range(a, b):
                act(i)
        else:
            def body(i, c):
                act(i)
                return c
            lax.fori_loop(a, b, body, 0)


def enter(n_sp, n_fs, n_tp):
    sp, fs, tp = (lax.axis_index(a) for a in ("sp", "fs", "tp"))
    barrier = pltpu.get_barrier_semaphore()
    bits = share_bits(n_fs)

    def greet(where):
        pl.semaphore_signal(barrier, inc=1, device_id=where, device_id_type=MESH)
    right, left = sp < n_sp - 1, sp > 0
    pl.when(right)(lambda: greet({"sp": lax.rem(sp + 1, n_sp)}))
    pl.when(left)(lambda: greet({"sp": lax.rem(sp + n_sp - 1, n_sp)}))
    for bit in bits:
        greet({"fs": fs + bit * (1 - 2 * (fs // bit % 2))})
    for d in range(1, n_tp):
        greet({"tp": lax.rem(tp + d, n_tp)})
    heard = len(bits) + n_tp - 1
    pl.semaphore_wait(barrier, heard + right.astype(jnp.int32) + left.astype(jnp.int32))


class Tokens:
    def __init__(self, n_sp, n_tp, tokbuf, rows, tok_s, tok_r, halo_s, halo_r):
        self.n_sp, self.n_tp, self.tokbuf, self.rows = n_sp, n_tp, tokbuf, rows
        self.tok_s, self.tok_r, self.halo_s, self.halo_r = tok_s, tok_r, halo_s, halo_r
        self.sp, self.tp = lax.axis_index("sp"), lax.axis_index("tp")
        self.end = n_tp - 1

    def tok_copy(self, d, owner):
        ref = self.tokbuf.at[pl.ds(pl.multiple_of(halo + owner * self.rows, 16), self.rows)]
        return pltpu.make_async_remote_copy(
            src_ref=ref, dst_ref=ref, send_sem=self.tok_s.at[d - 1], recv_sem=self.tok_r.at[d - 1],
            device_id={"tp": lax.rem(self.tp + d, self.n_tp)}, device_id_type=MESH)

    def halo_next(self):
        return pltpu.make_async_remote_copy(
            src_ref=self.tokbuf.at[pl.ds(self.n_tp * self.rows, halo)], dst_ref=self.tokbuf.at[pl.ds(0, halo)],
            send_sem=self.halo_s.at[0], recv_sem=self.halo_r.at[0],
            device_id={"sp": lax.rem(self.sp + 1, self.n_sp)}, device_id_type=MESH)

    def halo_side(self, d):
        ref = self.tokbuf.at[pl.ds(0, halo)]
        return pltpu.make_async_remote_copy(
            src_ref=ref, dst_ref=ref, send_sem=self.halo_s.at[d], recv_sem=self.halo_r.at[d],
            device_id={"tp": lax.rem(self.tp + d, self.n_tp)}, device_id_type=MESH)

    def start(self):
        for d in range(1, self.n_tp):
            self.tok_copy(d, self.tp).start()

    def start_halo(self):
        @pl.when(jnp.logical_and(self.tp == self.end, self.sp < self.n_sp - 1))
        def _():
            self.halo_next().start()

        @pl.when(self.sp == 0)
        def _():
            self.tokbuf[0:halo, :] = jnp.zeros((halo, self.tokbuf.shape[1]), self.tokbuf.dtype)

    def relay(self):
        @pl.when(jnp.logical_and(self.tp == self.end, self.sp > 0))
        def _():
            self.halo_next().wait_recv()
            for d in range(1, self.n_tp):
                self.halo_side(d).start()

    def finish(self):
        for d in range(1, self.n_tp):
            self.tok_copy(d, lax.rem(self.tp - d + self.n_tp, self.n_tp)).wait_recv()

        @pl.when(jnp.logical_and(self.tp < self.end, self.sp > 0))
        def _():
            for d in range(1, self.n_tp):
                @pl.when(self.tp == d - 1)
                def _():
                    self.halo_side(d).wait_recv()

    def drain(self):
        for d in range(1, self.n_tp):
            self.tok_copy(d, self.tp).wait_send()

        @pl.when(jnp.logical_and(self.tp == self.end, self.sp < self.n_sp - 1))
        def _():
            self.halo_next().wait_send()

        @pl.when(jnp.logical_and(self.tp == self.end, self.sp > 0))
        def _():
            for d in range(1, self.n_tp):
                self.halo_side(d).wait_send()


def mixer_kernel(n_sp, n_fs, n_tp, *refs):
    tok_ref, gain_ref, wbd_ref, conv_ref, alog_ref, extra_ref, mix_ref, scale_ref, dgain_ref = refs[:9]
    w_refs = refs[9:16]
    out_ref = refs[16]
    (tokbuf, normbuf, wbuf, raw, pool_out, delta_out, pbuf, cbuf, s_in, s_out, part, rsbuf,
     kbuf, xbuf, kwbuf, fbuf, qbuf, sbuf, gbuf, acc,
     loc, tok_s, tok_r, halo_s, halo_r, z_s, z_f, z_r, f_s, f_r, last_r, st_s, st_r, rs_s, rs_r) = refs[17:]
    rows, width = tok_ref.shape
    length = n_tp * rows
    heads, head_dim = cbuf.shape[0], cbuf.shape[1]
    groups, group_dim = mix_ref.shape[0], mix_ref.shape[1]
    sp, tp = lax.axis_index("sp"), lax.axis_index("tp")
    count = len(w_refs)
    cols = wbuf.shape[3]
    depth = wbuf.shape[2]
    local = [pltpu.make_async_copy(w_refs[i], wbuf.at[i, sp], loc.at[i]) for i in range(count)]
    here = pltpu.make_async_copy(
        tok_ref, tokbuf.at[pl.ds(pl.multiple_of(halo + tp * rows, 16), rows)], loc.at[count])
    local[0].start()
    here.start()
    for copy in local[1:]:
        copy.start()
    enter(n_sp, n_fs, n_tp)
    tokens = Tokens(n_sp, n_tp, tokbuf, rows, tok_s, tok_r, halo_s, halo_r)
    gather = Gather(n_sp, n_fs, wbuf, z_s, z_f, z_r, f_s, f_r, last_r)
    span = gather.span
    local[0].wait()
    gather.send(0)
    here.wait()
    tokens.start()
    for w in range(1, count):
        local[w].wait()
        if w < AHEAD:
            gather.send(w)
    tokens.start_halo()

    def norm(a, b):
        def body(i, c):
            at = pl.ds(pl.multiple_of(i * 16, 16), 16)
            normbuf[at, :] = rms_rows(tokbuf[at, :], gain_ref[...])
            return c
        lax.fori_loop(a, b, body, 0)

    def project(w):
        total = None
        for s in range(n_sp):
            term = jnp.dot(normbuf[:, s * depth:(s + 1) * depth], wbuf[w, s], preferred_element_type=f32)
            total = term if total is None else total + term
        raw[w] = total.astype(bf16).astype(f32)

    def active(role, w, h):
        at = slice(h * head_dim, (h + 1) * head_dim)
        taps = conv_ref.shape[1]
        total = None
        for j in range(taps):
            term = raw[w, pl.ds(halo - (taps - 1) + j, length), at] * conv_ref[role, j:j + 1, at]
            total = term if total is None else total + term
        return silu(total)

    unit = min(PAIR, length)
    per = length // unit
    i2 = lax.broadcasted_iota(jnp.int32, (unit, unit), 0)
    j2 = lax.broadcasted_iota(jnp.int32, (unit, unit), 1)
    lower = (i2 // BLOCK == j2 // BLOCK) & (i2 >= j2)
    strict = lower & (i2 > j2)

    def gates():
        pre = jnp.dot(normbuf[...], wbd_ref[...], preferred_element_type=f32)[halo:]
        softplus = jnp.maximum(pre, 0.0) + jnp.log1p(jnp.exp(-jnp.abs(pre)))
        log_gate = -jnp.exp(alog_ref[...]) * softplus + extra_ref[...]
        row = lax.broadcasted_iota(jnp.int32, (length, length), 0)
        col = lax.broadcasted_iota(jnp.int32, (length, length), 1)
        tri = jnp.where((row // BLOCK == col // BLOCK) & (row >= col), 1.0, 0.0)
        cum = mm(tri, log_gate)
        gbuf[0] = jax.nn.sigmoid(pre)
        gbuf[1] = cum
        cum_t = cum.T
        for p in range(per):
            for h in range(heads):
                at = slice(p * unit, (p + 1) * unit)
                gaps = cum[at, h:h + 1] - cum_t[h:h + 1, at]
                sbuf[h, p] = jnp.where(lower, jnp.exp(jnp.where(lower, gaps, 0.0)), 0.0)

    def keys(some):
        eye = jnp.where(i2 == j2, 1.0, 0.0)
        units = []
        for h in some:
            k = unit_rows(active(1, KEY, h))
            kb = k * gbuf[0, :, heads + h:heads + h + 1]
            kbuf[h] = k
            for p in range(per):
                at = slice(p * unit, (p + 1) * unit)
                corr = jnp.where(strict, mm(kb[at], k[at], ((1,), (1,))) * sbuf[h, p], 0.0)
                units.append((h, p, corr))
            kwbuf[h] = kb * jnp.exp(gbuf[1, :, h:h + 1])
        done = [eye - jnp.where(i2 // 2 == j2 // 2, u[2], 0.0) for u in units]
        size = 2
        while size < BLOCK:
            pair = (i2 // (2 * size) == j2 // (2 * size)) & (i2 // size != j2 // size)
            half = [mm(jnp.where(pair, u[2], 0.0), x) for u, x in zip(units, done)]
            done = [x - mm(x, y) for x, y in zip(done, half)]
            size *= 2
        for (h, p, _), x in zip(units, done):
            at = slice(p * unit, (p + 1) * unit)
            xbuf[h, p] = x
            kwbuf[h, at] = mm(x, kwbuf[h, at])

    def queries(some):
        for h in some:
            q = unit_rows(active(0, QUERY, h)) * head_dim ** (-0.5)
            qbuf[h] = q * jnp.exp(gbuf[1, :, h:h + 1])
            for p in range(per):
                at = slice(p * unit, (p + 1) * unit)
                sbuf[h, p] = mm(q[at], kbuf[h, at], ((1,), (1,))) * sbuf[h, p]

    def values(some):
        for h in some:
            vb = active(2, VALUE, h) * gbuf[0, :, heads + h:heads + h + 1]
            for p in range(per):
                at = slice(p * unit, (p + 1) * unit)
                fbuf[h, at] = mm(xbuf[h, p], vb[at])

    def scan():
        blank = jnp.concatenate([jnp.where(
            lax.broadcasted_iota(jnp.int32, (head_dim, head_dim), 0)
            == lax.broadcasted_iota(jnp.int32, (head_dim, head_dim), 1), 1.0, 0.0),
            jnp.zeros((head_dim, head_dim), f32)], axis=1)
        for p in range(per):
            for b in range(unit // BLOCK):
                at = slice(p * unit + b * BLOCK, p * unit + (b + 1) * BLOCK)
                sub = slice(b * BLOCK, (b + 1) * BLOCK)
                for h in range(heads):
                    fixed = fbuf[h, at]
                    g = gbuf[1, at, h:h + 1]
                    last = g[BLOCK - 1:BLOCK]
                    fall = kbuf[h, at] * jnp.exp(last - g)
                    c = blank if p + b == 0 else cbuf[h]
                    two = mm(jnp.concatenate([kwbuf[h, at], qbuf[h, at]], axis=0), c, precision=None)
                    fresh = jnp.concatenate([jnp.zeros_like(fixed), fixed], axis=1) - two[:BLOCK]
                    pbuf[h, at, :] = two[BLOCK:] + mm(sbuf[h, p, sub, sub], fresh, precision=None)
                    cbuf[h] = jnp.exp(last) * c + mm(fall, fresh, ((0,), (0,)), None)

    def pool():
        at_row = lax.broadcasted_iota(jnp.int32, (length, group_dim), 0) + sp * length
        for i in range(groups):
            at = slice(i * group_dim, (i + 1) * group_dim)
            x = raw[POOL, :, at]
            span_of = 2 * jnp.left_shift(1, lax.rem(tp * groups + i, 4))
            total = x
            window = jnp.zeros_like(x)
            for w in (2, 4, 8, 16):
                total = total + pltpu.roll(total, w // 2, 0)
                window = window + jnp.where(span_of == w, total, 0.0)
            tally = jnp.minimum(at_row + 1, span_of).astype(f32)
            pooled = (window[halo:] / tally - x[halo:]).astype(bf16)
            mixed = jnp.dot(pooled, mix_ref[i], preferred_element_type=f32)
            pool_out[:, at] = (mixed * scale_ref[:, at]).astype(bf16)

    def state_copy(h):
        return pltpu.make_async_remote_copy(
            src_ref=s_out.at[h], dst_ref=s_in.at[h], send_sem=st_s.at[h], recv_sem=st_r.at[h],
            device_id={"sp": lax.rem(sp + 1, n_sp)}, device_id_type=MESH)

    def relay():
        for h in range(heads):
            @pl.when(sp > 0)
            def _():
                state_copy(h).wait_recv()

            @pl.when(sp < n_sp - 1)
            def _():
                s_out[h] = (mm(cbuf[h, :, :head_dim], s_in[h].astype(f32), precision=None)
                            + cbuf[h, :, head_dim:]).astype(bf16)
                state_copy(h).start()

    def attend():
        for h in range(heads):
            at = slice(h * head_dim, (h + 1) * head_dim)
            attended = mm(pbuf[h, :, :head_dim], s_in[h].astype(f32), precision=None) + pbuf[h, :, head_dim:]
            scale = lax.rsqrt(jnp.mean(attended * attended, axis=-1, keepdims=True) + eps)
            delta_out[:, at] = (attended * scale * dgain_ref[...] * silu(raw[GATE, halo:, at])).astype(bf16)

    first = 4 * span

    def turn(r):
        return first + 7 * r // 3

    def plain(i):
        gather.step(i)

    def relaying(i):
        gather.step(i)
        if isinstance(i, int):
            for r in range(n_sp):
                if turn(r) == i:
                    pl.when(sp == r)(relay)
        else:
            pl.when(i == turn(sp))(relay)

    def advance(a, b):
        gather.loop(a, b, plain)

    half = (heads + 1) // 2
    low = halo // 16 + tp * (rows // 16)
    high = low + rows // 16
    first_part, second_part = range(half), range(half, heads)

    @pl.when(sp == 0)
    def _():
        s_in[...] = jnp.zeros_like(s_in)
    advance(0, 1)
    norm(low, high)
    advance(1, span)
    tokens.relay()
    advance(span, span + 1)
    tokens.finish()
    norm(0, low)
    norm(high, tokbuf.shape[0] // 16)
    gates()
    at = span + LAG
    advance(span + 1, at)
    gather.finish(KEY)
    project(KEY)
    keys(first_part)
    advance(at, at + 1)
    keys(second_part)
    advance(at + 1, 2 * span + LAG)
    gather.finish(QUERY)
    project(QUERY)
    queries(range(heads))
    gather.drain(KEY)
    advance(2 * span + LAG, 3 * span + LAG)
    gather.finish(VALUE)
    project(VALUE)
    values(range(heads))
    gather.drain(QUERY)
    scan()
    gather.loop(3 * span + LAG, 4 * span + LAG, relaying)
    gather.finish(POOL)
    project(POOL)
    pool()
    gather.drain(VALUE)
    gather.loop(4 * span + LAG, 5 * span + LAG, relaying)
    gather.finish(GATE)
    project(GATE)
    gather.drain(POOL)
    tokens.drain()
    gather.loop(5 * span + LAG, gather.steps(), relaying)
    attend()
    gather.drain(GATE)

    def rs_copy(s, d, owner, dest):
        return pltpu.make_async_remote_copy(
            src_ref=part.at[s, pl.ds(pl.multiple_of(dest * rows, 16), rows)], dst_ref=rsbuf.at[s, owner],
            send_sem=rs_s.at[s, d - 1], recv_sem=rs_r.at[s, d - 1],
            device_id={"tp": lax.rem(tp + d, n_tp)}, device_id_type=MESH)

    def product(s):
        part[s] = (acc[s] + jnp.dot(delta_out[...], wbuf[OUT_DELTA, s], preferred_element_type=f32)).astype(bf16)
        for d in range(1, n_tp):
            rs_copy(s, d, tp, lax.rem(tp + d, n_tp)).start()

    def collect(s):
        total = part[s, pl.ds(pl.multiple_of(tp * rows, 16), rows)].astype(f32)
        for d in range(1, n_tp):
            owner = lax.rem(tp - d + n_tp, n_tp)
            rs_copy(s, d, owner, tp).wait_recv()
            total = total + rsbuf[s, owner].astype(f32)
        out_ref[:, pl.ds(pl.multiple_of(s * cols, cols), cols)] = total.astype(bf16)

    gather.finish(OUT_POOL)

    def pool_product(s):
        acc[s] = jnp.dot(pool_out[...], wbuf[OUT_POOL, s], preferred_element_type=f32)
    gather.loop(0, n_sp, pool_product)
    product(sp)
    advance(gather.steps(), gather.end())

    def arrive(t):
        gather.ready(OUT_DELTA, t)
        gather.each(t, lambda src, way: product(src))
    gather.loop(1, n_sp, arrive)
    gather.drain(OUT_POOL)

    @pl.when(sp < n_sp - 1)
    def _():
        for h in range(heads):
            state_copy(h).wait_send()
    collect(sp)
    gather.loop(1, n_sp, lambda t: gather.each(t, lambda src, way: collect(src)))
    gather.drain(OUT_DELTA)

    def sent(s):
        for d in range(1, n_tp):
            rs_copy(s, d, tp, lax.rem(tp + d, n_tp)).wait_send()
    gather.loop(0, n_sp, sent)


def per_device(
    tokens,
    norm_gain,
    w_pool_in,
    w_query,
    w_key,
    w_value,
    w_gate,
    w_beta,
    w_decay,
    conv_weight,
    a_log,
    decay_extra,
    w_mix,
    pool_scale,
    delta_gain,
    w_out_pool,
    w_out_delta,
):
    n_sp, n_fs, n_tp = (lax.axis_size(a) for a in ("sp", "fs", "tp"))
    weights = (w_key, w_query, w_value, w_pool_in, w_gate, w_out_pool, w_out_delta)
    rows, width = tokens.shape
    depth, cols = w_key.shape
    heads = a_log.shape[0]
    head_dim = cols // heads
    length = n_tp * rows
    unit = min(PAIR, length)
    count = len(weights)
    lanes = 128
    lane = lax.axis_index("tp")

    def own(w):
        return lax.dynamic_slice_in_dim(w, lane * heads, heads, 1)

    def wide(x):
        return jnp.pad(x, ((0, 0), (0, lanes - x.shape[1])))

    w_bd = wide(jnp.concatenate([own(w_decay), own(w_beta)], axis=1))
    slots = max(1, 2 ** max(0, len(share_bits(n_fs)) - 1) - 1)
    side = max(1, n_tp - 1)
    dma = pltpu.SemaphoreType.DMA
    vmem, anywhere = pl.BlockSpec(memory_space=pltpu.VMEM), pl.BlockSpec(memory_space=pl.ANY)
    return pl.pallas_call(
        functools.partial(mixer_kernel, n_sp, n_fs, n_tp),
        out_shape=jax.ShapeDtypeStruct((rows, width), bf16),
        in_specs=[anywhere] + [vmem] * 8 + [anywhere] * count,
        out_specs=vmem,
        scratch_shapes=[
            pltpu.VMEM((halo + length, width), bf16),
            pltpu.VMEM((halo + length, width), bf16),
            pltpu.VMEM((count, n_sp, depth, cols), bf16),
            pltpu.VMEM((5, halo + length, cols), f32),
            pltpu.VMEM((length, cols), bf16),
            pltpu.VMEM((length, cols), bf16),
            pltpu.VMEM((heads, length, 2 * head_dim), f32),
            pltpu.VMEM((heads, head_dim, 2 * head_dim), f32),
            pltpu.VMEM((heads, head_dim, head_dim), bf16),
            pltpu.VMEM((heads, head_dim, head_dim), bf16),
            pltpu.VMEM((n_sp, length, cols), bf16),
            pltpu.VMEM((n_sp, n_tp, rows, cols), bf16),
            pltpu.VMEM((heads, length, head_dim), f32),
            pltpu.VMEM((heads, length // unit, unit, unit), f32),
            pltpu.VMEM((heads, length, head_dim), f32),
            pltpu.VMEM((heads, length, head_dim), f32),
            pltpu.VMEM((heads, length, head_dim), f32),
            pltpu.VMEM((heads, length // unit, unit, unit), f32),
            pltpu.VMEM((2, length, lanes), f32),
            pltpu.VMEM((n_sp, length, cols), f32),
            dma((count + 1,)), dma((side,)), dma((side,)), dma((n_tp,)), dma((n_tp,)),
            dma((count, 2)), dma((count,)), dma((count, n_sp)), dma((count,)), dma((count, n_sp, slots)),
            dma((count, n_sp)), dma((heads,)), dma((heads,)), dma((n_sp, side)), dma((n_sp, side)),
        ],
        compiler_params=pltpu.CompilerParams(collective_id=0, has_side_effects=True, vmem_limit_bytes=56 << 20),
    )(tokens, norm_gain.reshape(1, -1), w_bd, conv_weight, wide(a_log.reshape(1, -1)), wide(decay_extra), w_mix,
      pool_scale.reshape(1, -1), delta_gain.reshape(1, -1), *weights)


def solution(mesh):
    placed = (
        P(("fs", "sp", "tp"), None),
        P(),
        P("sp", "tp"),
        P("sp", "tp"),
        P("sp", "tp"),
        P("sp", "tp"),
        P("sp", "tp"),
        P(),
        P(),
        P(None, None, "tp"),
        P("tp"),
        P(("fs", "sp"), "tp"),
        P("tp", None, None),
        P("tp"),
        P(),
        P("tp", "sp"),
        P("tp", "sp"),
    )
    return jax.shard_map(
        per_device,
        mesh=mesh,
        in_specs=placed,
        out_specs=P(("fs", "sp", "tp"), None),
        check_vma=False,
    )
```

```python
import functools

import jax
import jax.numpy as jnp
from jax import lax
from jax.experimental import pallas as pl
from jax.experimental.pallas import tpu as pltpu
from jax.sharding import PartitionSpec as P

BLOCK = 64
PAIR = 2 * BLOCK

eps = 1e-06
halo = 16
MESH = pl.DeviceIdType.MESH
highest = lax.Precision.HIGHEST
f32 = jnp.float32
bf16 = jnp.bfloat16
KEY, QUERY, VALUE, GATE, POOL, OUT_POOL, OUT_DELTA = range(7)
AHEAD = 2
SKEW = 2.0
EARLY = 1.5
FINAL = 1.1
LAG = 2
UNROLL = 32


def mm(a, b, dims=((1,), (0,)), precision=highest):
    return lax.dot_general(a, b, (dims, ((), ())), precision=precision, preferred_element_type=f32)


def halves(a):
    high = a.astype(bf16)
    return high, (a - high.astype(f32)).astype(bf16)


def mm3(a, b, dims=((1,), (0,))):
    (a_high, a_low), (b_high, b_low) = a, b
    return (mm(a_high, b_high, dims, None) + mm(a_high, b_low, dims, None)) + mm(a_low, b_high, dims, None)


def rms_rows(values, gain):
    floats = values.astype(f32)
    scale = lax.rsqrt(jnp.mean(floats * floats, axis=-1, keepdims=True) + eps)
    return (floats * scale * gain.astype(f32)).astype(bf16)


def unit_rows(values):
    return values * lax.rsqrt(jnp.sum(values * values, axis=-1, keepdims=True) + eps)


def silu(x):
    return x * jax.nn.sigmoid(x)


def share_bits(n_fs):
    if n_fs & (n_fs - 1):
        return []
    return [n_fs >> (k + 1) for k in range(n_fs.bit_length() - 1)]


def both(a, b):
    if isinstance(a, bool):
        return b if a else False
    if isinstance(b, bool):
        return a if b else False
    return jnp.logical_and(a, b)


def when(cond, act):
    if isinstance(cond, bool):
        if cond:
            act()
    else:
        pl.when(cond)(act)


class Gather:
    def __init__(self, n_sp, n_fs, wbuf, z_s, z_f, z_r, f_s, f_r, last_r):
        self.n_sp, self.bits = n_sp, share_bits(n_fs)
        self.wbuf, self.z_s, self.z_f, self.z_r, self.f_s, self.f_r, self.last_r = wbuf, z_s, z_f, z_r, f_s, f_r, last_r
        self.sp, self.fs = lax.axis_index("sp"), lax.axis_index("fs")
        self.count = wbuf.shape[0]
        self.span = n_sp - 1
        self.pieces = 2 ** len(self.bits)
        self.mine = self.fs if self.bits else 0 * self.fs
        self.depth = wbuf.shape[2] // self.pieces
        self.plan_order()

    def partner(self, bit):
        return self.fs + bit * (1 - 2 * (self.fs // bit % 2))

    def mask_of(self, m, index):
        for i, bit in enumerate(self.bits):
            if m >> i & 1:
                index = index + bit * (1 - 2 * (index // bit % 2))
        return index

    def piece(self, w, src, index):
        return self.wbuf.at[w, src, pl.ds(pl.multiple_of(index * self.depth, self.depth), self.depth)]

    def z_copy(self, w, src, way, own):
        ref = self.piece(w, src, self.mine)
        to = lax.rem(self.sp + way + self.n_sp, self.n_sp)
        sent = self.z_s.at[w, (way + 1) // 2] if own else self.z_f.at[w]
        return pltpu.make_async_remote_copy(
            src_ref=ref, dst_ref=ref, send_sem=sent, recv_sem=self.z_r.at[w, src],
            device_id={"sp": to}, device_id_type=MESH)

    def f_copy(self, w, src, k, m):
        ref = self.piece(w, src, self.mask_of(m, self.mine))
        inner = k < len(self.bits) - 1
        return pltpu.make_async_remote_copy(
            src_ref=ref, dst_ref=ref, send_sem=self.f_s.at[w],
            recv_sem=self.f_r.at[w, src, 2 ** k - 1 + m] if inner else self.last_r.at[w, src],
            device_id={"fs": self.partner(self.bits[k])}, device_id_type=MESH)

    def can_send(self, way):
        return self.sp < self.n_sp - 1 if way == 1 else self.sp > 0

    def send(self, w):
        for way in (1, -1):
            @pl.when(self.can_send(way))
            def _():
                self.z_copy(w, self.sp, way, True).start()

    def each(self, t, act):
        for way in (1, -1):
            src = self.sp - way * t
            @pl.when(src >= 0 if way == 1 else src < self.n_sp)
            def _():
                act(src, way)

    def arrive_z(self, w, src, way):
        self.z_copy(w, src, way, False).wait_recv()

        @pl.when(self.can_send(way))
        def _():
            self.z_copy(w, src, way, False).start()
        for k in range(len(self.bits)):
            self.f_copy(w, src, k, 0).start()

    def arrive_f(self, w, t, k):
        def act(src, way):
            for m in range(2 ** k):
                self.f_copy(w, src, k, m).wait_recv()
                for later in range(k + 1, len(self.bits)):
                    self.f_copy(w, src, later, m | 1 << k).start()
        self.each(t, act)

    def steps(self):
        return self.count * self.span

    def plan_order(self):
        span, count = self.span, self.count
        if self.steps() > UNROLL:
            self.order, self.sends = None, None
            return
        key = {(w, t): (max(0.0, w * span - (w > 0) * EARLY - (w == count - 1) * FINAL) + SKEW * (t - 1), w) for w in range(count) for t in range(1, span + 1)}
        self.order = sorted(key, key=key.get)
        self.sends = {}
        for w in range(count):
            i = self.order.index((w, 1)) if span else 0
            while i > 0 and self.order[i - 1][1] == 1:
                i -= 1
            before = self.order[i - 1] if i > 0 else None
            at = -1 if before is None or w < AHEAD else self.order.index((before[0], before[1] - 1))
            self.sends.setdefault(at, []).append(w)

    def place(self, w, t):
        return self.order.index((w, t)) if self.order else w * self.span + t - 1

    def pair(self, i):
        if self.order:
            return self.order[min(i, len(self.order) - 1)]
        return i // self.span, i % self.span + 1

    def early(self):
        return self.sends.get(-1, []) if self.order else list(range(AHEAD))

    def step(self, i):
        if isinstance(i, int) and i < 0:
            return
        w, t = self.pair(i)
        when(i < self.steps(), lambda: self.each(t, lambda src, way: self.arrive_z(w, src, way)))
        if self.order:
            for later in self.sends.get(i, []):
                self.send(later)
        else:
            when(both(t == 1, w + AHEAD < self.count), lambda: self.send(w + AHEAD))
        for k in range(len(self.bits) - 1):
            j = i - LAG * (k + 1)

            def inner():
                w, t = self.pair(j)
                self.arrive_f(w, t, k)
            when(both(j >= 0, j < self.steps()), inner)

    def end(self):
        return self.steps() + LAG * max(0, len(self.bits) - 1)

    def ready(self, w, t):
        if self.bits:
            def act(src, way):
                ref = self.wbuf.at[w, src, pl.ds(0, self.wbuf.shape[2] // 2)]
                pltpu.make_async_copy(ref, ref, self.last_r.at[w, src]).wait()
            self.each(t, act)

    def finish(self, w):
        self.loop(1, self.n_sp, lambda t: self.ready(w, t))

    def drain(self, w):
        for way in (1, -1):
            @pl.when(self.can_send(way))
            def _():
                self.z_copy(w, self.sp, way, True).wait_send()
        if self.n_sp > 2:
            @pl.when(jnp.logical_and(self.can_send(1), self.can_send(-1)))
            def _():
                ref = self.wbuf.at[w, pl.ds(0, self.span), pl.ds(0, self.depth)]
                pltpu.make_async_copy(ref, ref, self.z_f.at[w]).wait()
        if self.bits:
            ref = self.wbuf.at[w, pl.ds(0, self.span), pl.ds(0, (self.pieces - 1) * self.depth)]
            pltpu.make_async_copy(ref, ref, self.f_s.at[w]).wait()

    def loop(self, a, b, act):
        if self.steps() <= UNROLL:
            for i in range(a, b):
                act(i)
        else:
            def body(i, c):
                act(i)
                return c
            lax.fori_loop(a, b, body, 0)


def enter(n_sp, n_fs, n_tp):
    sp, fs, tp = (lax.axis_index(a) for a in ("sp", "fs", "tp"))
    barrier = pltpu.get_barrier_semaphore()
    bits = share_bits(n_fs)

    def greet(where):
        pl.semaphore_signal(barrier, inc=1, device_id=where, device_id_type=MESH)
    right, left = sp < n_sp - 1, sp > 0
    pl.when(right)(lambda: greet({"sp": lax.rem(sp + 1, n_sp)}))
    pl.when(left)(lambda: greet({"sp": lax.rem(sp + n_sp - 1, n_sp)}))
    for bit in bits:
        greet({"fs": fs + bit * (1 - 2 * (fs // bit % 2))})
    for d in range(1, n_tp):
        greet({"tp": lax.rem(tp + d, n_tp)})
    pl.when(both(left, tp < n_tp - 1))(lambda: greet({"sp": lax.rem(sp + n_sp - 1, n_sp), "tp": n_tp - 1}))
    heard = len(bits) + n_tp - 1
    side = (n_tp - 1) * both(right, tp == n_tp - 1).astype(jnp.int32)
    pl.semaphore_wait(barrier, heard + right.astype(jnp.int32) + left.astype(jnp.int32) + side)


class Tokens:
    def __init__(self, n_sp, n_tp, tokbuf, rows, tok_s, tok_r, halo_s, halo_r):
        self.n_sp, self.n_tp, self.tokbuf, self.rows = n_sp, n_tp, tokbuf, rows
        self.tok_s, self.tok_r, self.halo_s, self.halo_r = tok_s, tok_r, halo_s, halo_r
        self.sp, self.tp = lax.axis_index("sp"), lax.axis_index("tp")
        self.end = n_tp - 1

    def tok_copy(self, d, owner):
        ref = self.tokbuf.at[pl.ds(pl.multiple_of(halo + owner * self.rows, 16), self.rows)]
        return pltpu.make_async_remote_copy(
            src_ref=ref, dst_ref=ref, send_sem=self.tok_s.at[d - 1], recv_sem=self.tok_r.at[d - 1],
            device_id={"tp": lax.rem(self.tp + d, self.n_tp)}, device_id_type=MESH)

    def halo_next(self, d):
        return pltpu.make_async_remote_copy(
            src_ref=self.tokbuf.at[pl.ds(self.n_tp * self.rows, halo)], dst_ref=self.tokbuf.at[pl.ds(0, halo)],
            send_sem=self.halo_s.at[d], recv_sem=self.halo_r.at[0],
            device_id={"sp": lax.rem(self.sp + 1, self.n_sp), "tp": lax.rem(self.tp + d, self.n_tp)},
            device_id_type=MESH)

    def start(self):
        for d in range(1, self.n_tp):
            self.tok_copy(d, self.tp).start()

    def start_halo(self):
        @pl.when(jnp.logical_and(self.tp == self.end, self.sp < self.n_sp - 1))
        def _():
            for d in range(self.n_tp):
                self.halo_next(d).start()

        @pl.when(self.sp == 0)
        def _():
            self.tokbuf[0:halo, :] = jnp.zeros((halo, self.tokbuf.shape[1]), self.tokbuf.dtype)

    def finish(self):
        for d in range(1, self.n_tp):
            self.tok_copy(d, lax.rem(self.tp - d + self.n_tp, self.n_tp)).wait_recv()

        @pl.when(self.sp > 0)
        def _():
            self.halo_next(0).wait_recv()

    def drain(self):
        for d in range(1, self.n_tp):
            self.tok_copy(d, self.tp).wait_send()

        @pl.when(jnp.logical_and(self.tp == self.end, self.sp < self.n_sp - 1))
        def _():
            for d in range(self.n_tp):
                self.halo_next(d).wait_send()


def mixer_kernel(n_sp, n_fs, n_tp, *refs):
    tok_ref, gain_ref, wb_ref, wd_ref, conv_ref, alog_ref, extra_ref, mix_ref, scale_ref, dgain_ref = refs[:10]
    w_refs = refs[10:17]
    out_ref = refs[17]
    (tokbuf, normbuf, wbuf, raw, pool_out, delta_out, pbuf, cbuf, s_in, s_out, part, rsbuf,
     kbuf, xbuf, ubuf, kwbuf, fbuf, qbuf, sbuf, gbuf, acc,
     loc, tok_s, tok_r, halo_s, halo_r, z_s, z_f, z_r, f_s, f_r, last_r, st_s, st_r, rs_s, rs_r) = refs[18:]
    rows, width = tok_ref.shape
    length = n_tp * rows
    heads, head_dim = cbuf.shape[0], cbuf.shape[1]
    groups, group_dim = mix_ref.shape[0], mix_ref.shape[1]
    sp, tp = lax.axis_index("sp"), lax.axis_index("tp")
    count = len(w_refs)
    cols = wbuf.shape[3]
    depth = wbuf.shape[2]
    local = [pltpu.make_async_copy(w_refs[i], wbuf.at[i, sp], loc.at[i]) for i in range(count)]
    here = pltpu.make_async_copy(
        tok_ref, tokbuf.at[pl.ds(pl.multiple_of(halo + tp * rows, 16), rows)], loc.at[count])
    local[0].start()
    here.start()
    for copy in local[1:]:
        copy.start()
    enter(n_sp, n_fs, n_tp)
    tokens = Tokens(n_sp, n_tp, tokbuf, rows, tok_s, tok_r, halo_s, halo_r)
    gather = Gather(n_sp, n_fs, wbuf, z_s, z_f, z_r, f_s, f_r, last_r)
    span = gather.span
    local[0].wait()
    gather.send(0)
    here.wait()
    tokens.start()
    for w in range(1, count):
        local[w].wait()
        if w in gather.early():
            gather.send(w)
    tokens.start_halo()

    def norm(a, b):
        def body(i, c):
            at = pl.ds(pl.multiple_of(i * 16, 16), 16)
            normbuf[at, :] = rms_rows(tokbuf[at, :], gain_ref[...].reshape(1, -1))
            return c
        lax.fori_loop(a, b, body, 0)

    def project(w):
        total = None
        for s in range(n_sp):
            term = jnp.dot(normbuf[:, s * depth:(s + 1) * depth], wbuf[w, s], preferred_element_type=f32)
            total = term if total is None else total + term
        raw[w] = total.astype(bf16).astype(f32)

    def active(role, w, h):
        at = slice(h * head_dim, (h + 1) * head_dim)
        taps = conv_ref.shape[1]
        total = None
        for j in range(taps):
            term = raw[w, pl.ds(halo - (taps - 1) + j, length), at] * conv_ref[role, j:j + 1, at]
            total = term if total is None else total + term
        return silu(total)

    unit = min(PAIR, length)
    per = length // unit
    i2 = lax.broadcasted_iota(jnp.int32, (unit, unit), 0)
    j2 = lax.broadcasted_iota(jnp.int32, (unit, unit), 1)
    lower = (i2 // BLOCK == j2 // BLOCK) & (i2 >= j2)
    strict = lower & (i2 > j2)

    def gates():
        lanes = gbuf.shape[2]
        total = wb_ref.shape[0]
        pick = jnp.where(
            lax.broadcasted_iota(jnp.int32, (total, lanes), 0)
            == tp * heads + lax.broadcasted_iota(jnp.int32, (total, lanes), 1), 1.0, 0.0)
        lane = lax.broadcasted_iota(jnp.int32, (1, lanes), 1)
        rate = jnp.zeros((1, lanes), f32)
        for h in range(heads):
            rate = jnp.where(lane == h, alog_ref[h], rate)
        keep = jnp.where(
            lax.broadcasted_iota(jnp.int32, (heads, lanes), 0)
            == lax.broadcasted_iota(jnp.int32, (heads, lanes), 1), 1.0, 0.0)

        def narrow(weight):
            return mm(mm(normbuf[...], weight, ((1,), (1,)), None)[halo:], pick)
        pre = narrow(wd_ref[...])
        softplus = jnp.maximum(pre, 0.0) + jnp.log1p(jnp.exp(-jnp.abs(pre)))
        log_gate = -jnp.exp(rate) * softplus + mm(extra_ref[...], keep, ((0,), (0,)))
        strength = narrow(wb_ref[...])
        row = lax.broadcasted_iota(jnp.int32, (length, length), 0)
        col = lax.broadcasted_iota(jnp.int32, (length, length), 1)
        tri = jnp.where((row // BLOCK == col // BLOCK) & (row >= col), 1.0, 0.0)
        cum = mm(tri, log_gate)
        gbuf[0] = jax.nn.sigmoid(strength)
        gbuf[1] = cum
        cum_t = cum.T
        for p in range(per):
            for h in range(heads):
                at = slice(p * unit, (p + 1) * unit)
                gaps = cum[at, h:h + 1] - cum_t[h:h + 1, at]
                sbuf[h, p] = jnp.where(lower, jnp.exp(jnp.where(lower, gaps, 0.0)), 0.0)

    all_units = [(h, p) for h in range(heads) for p in range(per)]

    def rows_of(p):
        return slice(p * unit, (p + 1) * unit)

    def keys(some):
        eye = jnp.where(i2 == j2, 1.0, 0.0)
        for h in some:
            k = unit_rows(active(1, KEY, h))
            kb = k * gbuf[0, :, h:h + 1]
            kbuf[h] = k
            for p in range(per):
                at = rows_of(p)
                corr = jnp.where(strict, mm3(halves(kb[at]), halves(k[at]), ((1,), (1,))) * sbuf[h, p], 0.0)
                ubuf[h, p] = corr
                xbuf[h, p] = eye - jnp.where(i2 // 2 == j2 // 2, corr, 0.0)
            kwbuf[h] = kb * jnp.exp(gbuf[1, :, h:h + 1])

    def level(size):
        pair = (i2 // (2 * size) == j2 // (2 * size)) & (i2 // size != j2 // size)
        done = {u: halves(xbuf[u]) for u in all_units}
        part_way = {u: mm3(halves(jnp.where(pair, ubuf[u], 0.0)), done[u]) for u in all_units}
        for u in all_units:
            xbuf[u] = xbuf[u] - mm3(done[u], halves(part_way[u]))

    def key_weights():
        for h, p in all_units:
            kwbuf[h, rows_of(p)] = mm3(halves(xbuf[h, p]), halves(kwbuf[h, rows_of(p)]))

    def queries(some):
        for h in some:
            q = unit_rows(active(0, QUERY, h)) * head_dim ** (-0.5)
            qbuf[h] = q * jnp.exp(gbuf[1, :, h:h + 1])
            for p in range(per):
                at = rows_of(p)
                sbuf[h, p] = mm3(halves(q[at]), halves(kbuf[h, at]), ((1,), (1,))) * sbuf[h, p]

    def values(some):
        for h in some:
            vb = active(2, VALUE, h) * gbuf[0, :, h:h + 1]
            for p in range(per):
                at = rows_of(p)
                fbuf[h, at] = mm3(halves(xbuf[h, p]), halves(vb[at]))

    def scan(some):
        blank = jnp.concatenate([jnp.where(
            lax.broadcasted_iota(jnp.int32, (head_dim, head_dim), 0)
            == lax.broadcasted_iota(jnp.int32, (head_dim, head_dim), 1), 1.0, 0.0),
            jnp.zeros((head_dim, head_dim), f32)], axis=1)
        for p in some:
            for b in range(unit // BLOCK):
                at = slice(p * unit + b * BLOCK, p * unit + (b + 1) * BLOCK)
                sub = slice(b * BLOCK, (b + 1) * BLOCK)
                for h in range(heads):
                    fixed = fbuf[h, at]
                    g = gbuf[1, at, h:h + 1]
                    last = g[BLOCK - 1:BLOCK]
                    fall = kbuf[h, at] * jnp.exp(last - g)
                    c = blank if p + b == 0 else cbuf[h]
                    two = mm(jnp.concatenate([kwbuf[h, at], qbuf[h, at]], axis=0), c, precision=None)
                    fresh = jnp.concatenate([jnp.zeros_like(fixed), fixed], axis=1) - two[:BLOCK]
                    pbuf[h, at, :] = two[BLOCK:] + mm(sbuf[h, p, sub, sub], fresh, precision=None)
                    cbuf[h] = jnp.exp(last) * c + mm(fall, fresh, ((0,), (0,)), None)

    def pool():
        at_row = lax.broadcasted_iota(jnp.int32, (length, group_dim), 0) + sp * length
        for i in range(groups):
            at = slice(i * group_dim, (i + 1) * group_dim)
            x = raw[POOL, :, at]
            span_of = 2 * jnp.left_shift(1, lax.rem(tp * groups + i, 4))
            total = x
            window = jnp.zeros_like(x)
            for w in (2, 4, 8, 16):
                total = total + pltpu.roll(total, w // 2, 0)
                window = window + jnp.where(span_of == w, total, 0.0)
            tally = jnp.minimum(at_row + 1, span_of).astype(f32)
            pooled = (window[halo:] / tally - x[halo:]).astype(bf16)
            mixed = jnp.dot(pooled, mix_ref[i], preferred_element_type=f32)
            pool_out[:, at] = (mixed * scale_ref[at].reshape(1, -1)).astype(bf16)

    def state_copy(h):
        return pltpu.make_async_remote_copy(
            src_ref=s_out.at[h], dst_ref=s_in.at[h], send_sem=st_s.at[h], recv_sem=st_r.at[h],
            device_id={"sp": lax.rem(sp + 1, n_sp)}, device_id_type=MESH)

    def relay():
        for h in range(heads):
            @pl.when(sp > 0)
            def _():
                state_copy(h).wait_recv()

            @pl.when(sp < n_sp - 1)
            def _():
                s_out[h] = (mm(cbuf[h, :, :head_dim], s_in[h].astype(f32), precision=None)
                            + cbuf[h, :, head_dim:]).astype(bf16)
                state_copy(h).start()

    def attend():
        for h in range(heads):
            at = slice(h * head_dim, (h + 1) * head_dim)
            attended = mm(pbuf[h, :, :head_dim], s_in[h].astype(f32), precision=None) + pbuf[h, :, head_dim:]
            scale = lax.rsqrt(jnp.mean(attended * attended, axis=-1, keepdims=True) + eps)
            delta_out[:, at] = (attended * scale * dgain_ref[...].reshape(1, -1) * silu(raw[GATE, halo:, at])).astype(bf16)

    def rs_copy(s, d, owner, dest):
        return pltpu.make_async_remote_copy(
            src_ref=part.at[s, pl.ds(pl.multiple_of(dest * rows, 16), rows)], dst_ref=rsbuf.at[s, owner],
            send_sem=rs_s.at[s, d - 1], recv_sem=rs_r.at[s, d - 1],
            device_id={"tp": lax.rem(tp + d, n_tp)}, device_id_type=MESH)

    def product(s):
        part[s] = (acc[s] + jnp.dot(delta_out[...], wbuf[OUT_DELTA, s], preferred_element_type=f32)).astype(bf16)
        for d in range(1, n_tp):
            rs_copy(s, d, tp, lax.rem(tp + d, n_tp)).start()

    def collect(s):
        total = part[s, pl.ds(pl.multiple_of(tp * rows, 16), rows)].astype(f32)
        for d in range(1, n_tp):
            owner = lax.rem(tp - d + n_tp, n_tp)
            rs_copy(s, d, owner, tp).wait_recv()
            total = total + rsbuf[s, owner].astype(f32)
        out_ref[:, pl.ds(pl.multiple_of(s * cols, cols), cols)] = total.astype(bf16)

    def pool_product(s):
        acc[s] = jnp.dot(pool_out[...], wbuf[OUT_POOL, s], preferred_element_type=f32)

    def ready(w):
        return max([gather.place(w, t) for t in range(1, n_sp)], default=0) + LAG

    turns = ready(VALUE) + 2

    def step(i):
        gather.step(i)
        if isinstance(i, int):
            for r in range(n_sp):
                if turns + 2 * r == i:
                    pl.when(sp == r)(relay)
        else:
            pl.when(i == turns + 2 * sp)(relay)

    half = (heads + 1) // 2
    middle = (per + 1) // 2
    low = halo // 16 + tp * (rows // 16)
    high = low + rows // 16
    left, right = range(half), range(half, heads)
    sizes = [2 << i for i in range((BLOCK // 2).bit_length() - 1)]

    @pl.when(sp == 0)
    def _():
        s_in[...] = jnp.zeros_like(s_in)

    def arrive_pool(t):
        gather.ready(OUT_POOL, t)
        gather.each(t, lambda src, way: pool_product(src))

    def arrive(t):
        gather.ready(OUT_DELTA, t)
        gather.each(t, lambda src, way: product(src))

    attend_at = max(turns + 2 * span, ready(POOL) + 2)
    plan = [
        (0, lambda: norm(low, high)),
        (span - 1, tokens.finish), (span - 1, lambda: norm(0, low)),
        (span, lambda: norm(high, tokbuf.shape[0] // 16)), (span, gates),
        (ready(KEY), lambda: gather.finish(KEY)), (ready(KEY), lambda: project(KEY)),
        (ready(KEY) + 1, lambda: keys(left)), (ready(KEY) + 1, lambda: keys(right)),
        (ready(QUERY), lambda: gather.finish(QUERY)), (ready(QUERY), lambda: project(QUERY)),
        (ready(QUERY) + 2, key_weights), (ready(QUERY) + 2, lambda: queries(left)),
        (ready(QUERY) + 2, lambda: gather.drain(KEY)), (ready(QUERY) + 2, lambda: queries(right)),
        (ready(VALUE), lambda: gather.finish(VALUE)), (ready(VALUE), lambda: project(VALUE)),
        (ready(VALUE), lambda: values(range(heads))), (ready(VALUE), lambda: scan(range(middle))),
        (ready(VALUE) + 1, lambda: scan(range(middle, per))), (ready(VALUE) + 1, lambda: gather.drain(QUERY)),
        (ready(GATE) + 1, lambda: gather.finish(GATE)), (ready(GATE) + 1, lambda: project(GATE)),
        (ready(GATE) + 1, lambda: gather.drain(VALUE)), (ready(GATE) + 1, tokens.drain),
        (ready(POOL), lambda: gather.finish(POOL)), (ready(POOL), lambda: project(POOL)),
        (ready(POOL) + 1, pool), (ready(POOL) + 1, lambda: gather.drain(GATE)),
        (ready(POOL) + 2, lambda: pool_product(sp)),
        (attend_at, attend), (attend_at, lambda: product(sp)), (attend_at, lambda: gather.drain(POOL)),
        (gather.end() - 1, lambda: None),
    ]
    where = [ready(KEY) + 2, ready(KEY) + 2, ready(QUERY), ready(QUERY) + 1, ready(QUERY) + 1]
    for n, size in enumerate(sizes):
        plan.append((where[min(n, len(where) - 1)], functools.partial(level, size)))
    for t in range(1, n_sp):
        pooled_at = gather.place(OUT_POOL, t) + LAG
        plan.append((max(ready(POOL) + 2, pooled_at), functools.partial(arrive_pool, t)))
        plan.append((max(attend_at, pooled_at, gather.place(OUT_DELTA, t) + LAG), functools.partial(arrive, t)))
    plan.sort(key=lambda entry: entry[0])
    reached = 0
    for at_step, act in plan:
        if at_step >= reached:
            gather.loop(reached, at_step + 1, step)
            reached = at_step + 1
        act()
    gather.drain(OUT_POOL)

    @pl.when(sp < n_sp - 1)
    def _():
        for h in range(heads):
            state_copy(h).wait_send()
    collect(sp)
    gather.loop(1, n_sp, lambda t: gather.each(t, lambda src, way: collect(src)))
    gather.drain(OUT_DELTA)

    def sent(s):
        for d in range(1, n_tp):
            rs_copy(s, d, tp, lax.rem(tp + d, n_tp)).wait_send()
    gather.loop(0, n_sp, sent)


def per_device(
    tokens,
    norm_gain,
    w_pool_in,
    w_query,
    w_key,
    w_value,
    w_gate,
    w_beta,
    w_decay,
    conv_weight,
    a_log,
    decay_extra,
    w_mix,
    pool_scale,
    delta_gain,
    w_out_pool,
    w_out_delta,
):
    n_sp, n_fs, n_tp = (lax.axis_size(a) for a in ("sp", "fs", "tp"))
    weights = (w_key, w_query, w_value, w_gate, w_pool_in, w_out_pool, w_out_delta)
    rows, width = tokens.shape
    depth, cols = w_key.shape
    heads = a_log.shape[0]
    head_dim = cols // heads
    length = n_tp * rows
    unit = min(PAIR, length)
    count = len(weights)
    lanes = 128
    slots = max(1, 2 ** max(0, len(share_bits(n_fs)) - 1) - 1)
    side = max(1, n_tp - 1)
    dma = pltpu.SemaphoreType.DMA
    vmem, anywhere = pl.BlockSpec(memory_space=pltpu.VMEM), pl.BlockSpec(memory_space=pl.ANY)
    scalars = pl.BlockSpec(memory_space=pltpu.SMEM)
    return pl.pallas_call(
        functools.partial(mixer_kernel, n_sp, n_fs, n_tp),
        out_shape=jax.ShapeDtypeStruct((rows, width), bf16),
        in_specs=[anywhere] + [vmem] * 4 + [scalars] + [vmem] * 4 + [anywhere] * count,
        out_specs=vmem,
        scratch_shapes=[
            pltpu.VMEM((halo + length, width), bf16),
            pltpu.VMEM((halo + length, width), bf16),
            pltpu.VMEM((count, n_sp, depth, cols), bf16),
            pltpu.VMEM((5, halo + length, cols), f32),
            pltpu.VMEM((length, cols), bf16),
            pltpu.VMEM((length, cols), bf16),
            pltpu.VMEM((heads, length, 2 * head_dim), f32),
            pltpu.VMEM((heads, head_dim, 2 * head_dim), f32),
            pltpu.VMEM((heads, head_dim, head_dim), bf16),
            pltpu.VMEM((heads, head_dim, head_dim), bf16),
            pltpu.VMEM((n_sp, length, cols), bf16),
            pltpu.VMEM((n_sp, n_tp, rows, cols), bf16),
            pltpu.VMEM((heads, length, head_dim), f32),
            pltpu.VMEM((heads, length // unit, unit, unit), f32),
            pltpu.VMEM((heads, length // unit, unit, unit), f32),
            pltpu.VMEM((heads, length, head_dim), f32),
            pltpu.VMEM((heads, length, head_dim), f32),
            pltpu.VMEM((heads, length, head_dim), f32),
            pltpu.VMEM((heads, length // unit, unit, unit), f32),
            pltpu.VMEM((2, length, lanes), f32),
            pltpu.VMEM((n_sp, length, cols), f32),
            dma((count + 1,)), dma((side,)), dma((side,)), dma((n_tp,)), dma((1,)),
            dma((count, 2)), dma((count,)), dma((count, n_sp)), dma((count,)), dma((count, n_sp, slots)),
            dma((count, n_sp)), dma((heads,)), dma((heads,)), dma((n_sp, side)), dma((n_sp, side)),
        ],
        compiler_params=pltpu.CompilerParams(collective_id=0, has_side_effects=True, vmem_limit_bytes=56 << 20),
    )(tokens, norm_gain, w_beta.T, w_decay.T, conv_weight, a_log, decay_extra.T, w_mix, pool_scale, delta_gain, *weights)


def solution(mesh):
    placed = (
        P(("fs", "sp", "tp"), None),
        P(),
        P("sp", "tp"),
        P("sp", "tp"),
        P("sp", "tp"),
        P("sp", "tp"),
        P("sp", "tp"),
        P(),
        P(),
        P(None, None, "tp"),
        P("tp"),
        P(("fs", "sp"), "tp"),
        P("tp", None, None),
        P("tp"),
        P(),
        P("tp", "sp"),
        P("tp", "sp"),
    )
    return jax.shard_map(
        per_device,
        mesh=mesh,
        in_specs=placed,
        out_specs=P(("fs", "sp", "tp"), None),
        check_vma=False,
    )
```

```python
import functools

import jax
import jax.numpy as jnp
from jax import lax
from jax.experimental import pallas as pl
from jax.experimental.pallas import tpu as pltpu
from jax.sharding import PartitionSpec as P

BLOCK = 64
PAIR = 2 * BLOCK

eps = 1e-06
halo = 16
MESH = pl.DeviceIdType.MESH
highest = lax.Precision.HIGHEST
f32 = jnp.float32
bf16 = jnp.bfloat16
KEY, QUERY, VALUE, GATE, POOL, OUT_POOL, OUT_DELTA = range(7)
AHEAD = 2
SKEW = 2.0
EARLY = 1.5
FINAL = 1.1
LAG = 2
UNROLL = 32


def mm(a, b, dims=((1,), (0,)), precision=highest):
    return lax.dot_general(a, b, (dims, ((), ())), precision=precision, preferred_element_type=f32)


def halves(a):
    high = a.astype(bf16)
    return high, (a - high.astype(f32)).astype(bf16)


def mm3(a, b, dims=((1,), (0,))):
    (a_high, a_low), (b_high, b_low) = a, b
    return (mm(a_high, b_high, dims, None) + mm(a_high, b_low, dims, None)) + mm(a_low, b_high, dims, None)


def rms_rows(values, gain):
    floats = values.astype(f32)
    scale = lax.rsqrt(jnp.mean(floats * floats, axis=-1, keepdims=True) + eps)
    return (floats * scale * gain.astype(f32)).astype(bf16)


def unit_rows(values):
    return values * lax.rsqrt(jnp.sum(values * values, axis=-1, keepdims=True) + eps)


def silu(x):
    return x * jax.nn.sigmoid(x)


def share_bits(n_fs):
    if n_fs & (n_fs - 1):
        return []
    return [n_fs >> (k + 1) for k in range(n_fs.bit_length() - 1)]


def both(a, b):
    if isinstance(a, bool):
        return b if a else False
    if isinstance(b, bool):
        return a if b else False
    return jnp.logical_and(a, b)


def when(cond, act):
    if isinstance(cond, bool):
        if cond:
            act()
    else:
        pl.when(cond)(act)


class Gather:
    def __init__(self, n_sp, n_fs, wbuf, z_s, z_f, z_r, f_s, f_r, last_r):
        self.n_sp, self.bits = n_sp, share_bits(n_fs)
        self.wbuf, self.z_s, self.z_f, self.z_r, self.f_s, self.f_r, self.last_r = wbuf, z_s, z_f, z_r, f_s, f_r, last_r
        self.sp, self.fs = lax.axis_index("sp"), lax.axis_index("fs")
        self.count = wbuf.shape[0]
        self.span = n_sp - 1
        self.pieces = 2 ** len(self.bits)
        self.mine = self.fs if self.bits else 0 * self.fs
        self.depth = wbuf.shape[2] // self.pieces
        self.plan_order()

    def partner(self, bit):
        return self.fs + bit * (1 - 2 * (self.fs // bit % 2))

    def mask_of(self, m, index):
        for i, bit in enumerate(self.bits):
            if m >> i & 1:
                index = index + bit * (1 - 2 * (index // bit % 2))
        return index

    def piece(self, w, src, index):
        return self.wbuf.at[w, src, pl.ds(pl.multiple_of(index * self.depth, self.depth), self.depth)]

    def z_copy(self, w, src, way, own):
        ref = self.piece(w, src, self.mine)
        to = lax.rem(self.sp + way + self.n_sp, self.n_sp)
        sent = self.z_s.at[w, (way + 1) // 2] if own else self.z_f.at[w]
        return pltpu.make_async_remote_copy(
            src_ref=ref, dst_ref=ref, send_sem=sent, recv_sem=self.z_r.at[w, src],
            device_id={"sp": to}, device_id_type=MESH)

    def f_copy(self, w, src, k, m):
        ref = self.piece(w, src, self.mask_of(m, self.mine))
        inner = k < len(self.bits) - 1
        return pltpu.make_async_remote_copy(
            src_ref=ref, dst_ref=ref, send_sem=self.f_s.at[w],
            recv_sem=self.f_r.at[w, src, 2 ** k - 1 + m] if inner else self.last_r.at[w, src],
            device_id={"fs": self.partner(self.bits[k])}, device_id_type=MESH)

    def can_send(self, way):
        return self.sp < self.n_sp - 1 if way == 1 else self.sp > 0

    def send(self, w):
        for way in (1, -1):
            @pl.when(self.can_send(way))
            def _():
                self.z_copy(w, self.sp, way, True).start()

    def each(self, t, act):
        for way in (1, -1):
            src = self.sp - way * t
            @pl.when(src >= 0 if way == 1 else src < self.n_sp)
            def _():
                act(src, way)

    def arrive_z(self, w, src, way):
        self.z_copy(w, src, way, False).wait_recv()

        @pl.when(self.can_send(way))
        def _():
            self.z_copy(w, src, way, False).start()
        for k in range(len(self.bits)):
            self.f_copy(w, src, k, 0).start()

    def arrive_f(self, w, t, k):
        def act(src, way):
            for m in range(2 ** k):
                self.f_copy(w, src, k, m).wait_recv()
                for later in range(k + 1, len(self.bits)):
                    self.f_copy(w, src, later, m | 1 << k).start()
        self.each(t, act)

    def steps(self):
        return self.count * self.span

    def plan_order(self):
        span, count = self.span, self.count
        if self.steps() > UNROLL:
            self.order, self.sends = None, None
            return
        key = {(w, t): (max(0.0, w * span - (w > 0) * EARLY - (w == count - 1) * FINAL) + SKEW * (t - 1), w) for w in range(count) for t in range(1, span + 1)}
        self.order = sorted(key, key=key.get)
        self.sends = {}
        for w in range(count):
            i = self.order.index((w, 1)) if span else 0
            while i > 0 and self.order[i - 1][1] == 1:
                i -= 1
            before = self.order[i - 1] if i > 0 else None
            at = -1 if before is None or w < AHEAD else self.order.index((before[0], before[1] - 1))
            self.sends.setdefault(at, []).append(w)

    def place(self, w, t):
        return self.order.index((w, t)) if self.order else w * self.span + t - 1

    def pair(self, i):
        if self.order:
            return self.order[min(i, len(self.order) - 1)]
        return i // self.span, i % self.span + 1

    def early(self):
        return self.sends.get(-1, []) if self.order else list(range(AHEAD))

    def step(self, i):
        if isinstance(i, int) and i < 0:
            return
        w, t = self.pair(i)
        when(i < self.steps(), lambda: self.each(t, lambda src, way: self.arrive_z(w, src, way)))
        if self.order:
            for later in self.sends.get(i, []):
                self.send(later)
        else:
            when(both(t == 1, w + AHEAD < self.count), lambda: self.send(w + AHEAD))
        for k in range(len(self.bits) - 1):
            j = i - LAG * (k + 1)

            def inner():
                w, t = self.pair(j)
                self.arrive_f(w, t, k)
            when(both(j >= 0, j < self.steps()), inner)

    def end(self):
        return self.steps() + LAG * max(0, len(self.bits) - 1)

    def ready(self, w, t):
        if self.bits:
            def act(src, way):
                ref = self.wbuf.at[w, src, pl.ds(0, self.wbuf.shape[2] // 2)]
                pltpu.make_async_copy(ref, ref, self.last_r.at[w, src]).wait()
            self.each(t, act)

    def finish(self, w):
        self.loop(1, self.n_sp, lambda t: self.ready(w, t))

    def drain(self, w):
        for way in (1, -1):
            @pl.when(self.can_send(way))
            def _():
                self.z_copy(w, self.sp, way, True).wait_send()
        if self.n_sp > 2:
            @pl.when(jnp.logical_and(self.can_send(1), self.can_send(-1)))
            def _():
                ref = self.wbuf.at[w, pl.ds(0, self.span), pl.ds(0, self.depth)]
                pltpu.make_async_copy(ref, ref, self.z_f.at[w]).wait()
        if self.bits:
            ref = self.wbuf.at[w, pl.ds(0, self.span), pl.ds(0, (self.pieces - 1) * self.depth)]
            pltpu.make_async_copy(ref, ref, self.f_s.at[w]).wait()

    def loop(self, a, b, act):
        if self.steps() <= UNROLL:
            for i in range(a, b):
                act(i)
        else:
            def body(i, c):
                act(i)
                return c
            lax.fori_loop(a, b, body, 0)


def enter(n_sp, n_fs, n_tp):
    sp, fs, tp = (lax.axis_index(a) for a in ("sp", "fs", "tp"))
    barrier = pltpu.get_barrier_semaphore()
    bits = share_bits(n_fs)

    def greet(where):
        pl.semaphore_signal(barrier, inc=1, device_id=where, device_id_type=MESH)
    right, left = sp < n_sp - 1, sp > 0
    pl.when(right)(lambda: greet({"sp": lax.rem(sp + 1, n_sp)}))
    pl.when(left)(lambda: greet({"sp": lax.rem(sp + n_sp - 1, n_sp)}))
    for bit in bits:
        greet({"fs": fs + bit * (1 - 2 * (fs // bit % 2))})
    for d in range(1, n_tp):
        greet({"tp": lax.rem(tp + d, n_tp)})
    pl.when(both(left, tp < n_tp - 1))(lambda: greet({"sp": lax.rem(sp + n_sp - 1, n_sp), "tp": n_tp - 1}))
    heard = len(bits) + n_tp - 1
    side = (n_tp - 1) * both(right, tp == n_tp - 1).astype(jnp.int32)
    pl.semaphore_wait(barrier, heard + right.astype(jnp.int32) + left.astype(jnp.int32) + side)


class Tokens:
    def __init__(self, n_sp, n_tp, tokbuf, rows, tok_s, tok_r, halo_s, halo_r):
        self.n_sp, self.n_tp, self.tokbuf, self.rows = n_sp, n_tp, tokbuf, rows
        self.tok_s, self.tok_r, self.halo_s, self.halo_r = tok_s, tok_r, halo_s, halo_r
        self.sp, self.tp = lax.axis_index("sp"), lax.axis_index("tp")
        self.end = n_tp - 1

    def tok_copy(self, d, owner):
        ref = self.tokbuf.at[pl.ds(pl.multiple_of(halo + owner * self.rows, 16), self.rows)]
        return pltpu.make_async_remote_copy(
            src_ref=ref, dst_ref=ref, send_sem=self.tok_s.at[d - 1], recv_sem=self.tok_r.at[d - 1],
            device_id={"tp": lax.rem(self.tp + d, self.n_tp)}, device_id_type=MESH)

    def halo_next(self, d):
        return pltpu.make_async_remote_copy(
            src_ref=self.tokbuf.at[pl.ds(self.n_tp * self.rows, halo)], dst_ref=self.tokbuf.at[pl.ds(0, halo)],
            send_sem=self.halo_s.at[d], recv_sem=self.halo_r.at[0],
            device_id={"sp": lax.rem(self.sp + 1, self.n_sp), "tp": lax.rem(self.tp + d, self.n_tp)},
            device_id_type=MESH)

    def start(self):
        for d in range(1, self.n_tp):
            self.tok_copy(d, self.tp).start()

    def start_halo(self):
        @pl.when(jnp.logical_and(self.tp == self.end, self.sp < self.n_sp - 1))
        def _():
            for d in range(self.n_tp):
                self.halo_next(d).start()

        @pl.when(self.sp == 0)
        def _():
            self.tokbuf[0:halo, :] = jnp.zeros((halo, self.tokbuf.shape[1]), self.tokbuf.dtype)

    def finish(self):
        for d in range(1, self.n_tp):
            self.tok_copy(d, lax.rem(self.tp - d + self.n_tp, self.n_tp)).wait_recv()

        @pl.when(self.sp > 0)
        def _():
            self.halo_next(0).wait_recv()

    def drain(self):
        for d in range(1, self.n_tp):
            self.tok_copy(d, self.tp).wait_send()

        @pl.when(jnp.logical_and(self.tp == self.end, self.sp < self.n_sp - 1))
        def _():
            for d in range(self.n_tp):
                self.halo_next(d).wait_send()


def mixer_kernel(n_sp, n_fs, n_tp, *refs):
    tok_ref, gain_ref, wb_ref, wd_ref, conv_ref, alog_ref, extra_ref, mix_ref, scale_ref, dgain_ref = refs[:10]
    w_refs = refs[10:17]
    out_ref = refs[17]
    (tokbuf, normbuf, wbuf, raw, pool_out, delta_out, pbuf, cbuf, s_in, s_out, part, rsbuf,
     kbuf, xbuf, ubuf, kwbuf, fbuf, qbuf, sbuf, gbuf, acc,
     loc, tok_s, tok_r, halo_s, halo_r, z_s, z_f, z_r, f_s, f_r, last_r, st_s, st_r, rs_s, rs_r) = refs[18:]
    rows, width = tok_ref.shape
    length = n_tp * rows
    heads, head_dim = cbuf.shape[0], cbuf.shape[1]
    groups, group_dim = mix_ref.shape[0], mix_ref.shape[1]
    sp, tp = lax.axis_index("sp"), lax.axis_index("tp")
    count = len(w_refs)
    cols = wbuf.shape[3]
    depth = wbuf.shape[2]
    local = [pltpu.make_async_copy(w_refs[i], wbuf.at[i, sp], loc.at[i]) for i in range(count)]
    here = pltpu.make_async_copy(
        tok_ref, tokbuf.at[pl.ds(pl.multiple_of(halo + tp * rows, 16), rows)], loc.at[count])
    local[0].start()
    here.start()
    for copy in local[1:]:
        copy.start()
    enter(n_sp, n_fs, n_tp)
    tokens = Tokens(n_sp, n_tp, tokbuf, rows, tok_s, tok_r, halo_s, halo_r)
    gather = Gather(n_sp, n_fs, wbuf, z_s, z_f, z_r, f_s, f_r, last_r)
    span = gather.span
    local[0].wait()
    gather.send(0)
    here.wait()
    tokens.start()
    for w in range(1, count):
        local[w].wait()
        if w in gather.early():
            gather.send(w)
    tokens.start_halo()

    def norm(a, b):
        def body(i, c):
            at = pl.ds(pl.multiple_of(i * 16, 16), 16)
            normbuf[at, :] = rms_rows(tokbuf[at, :], gain_ref[...].reshape(1, -1))
            return c
        lax.fori_loop(a, b, body, 0)

    def project(w):
        total = None
        for s in range(n_sp):
            term = jnp.dot(normbuf[:, s * depth:(s + 1) * depth], wbuf[w, s], preferred_element_type=f32)
            total = term if total is None else total + term
        raw[w] = total.astype(bf16).astype(f32)

    def active(role, w, h):
        at = slice(h * head_dim, (h + 1) * head_dim)
        taps = conv_ref.shape[1]
        total = None
        for j in range(taps):
            term = raw[w, pl.ds(halo - (taps - 1) + j, length), at] * conv_ref[role, j:j + 1, at]
            total = term if total is None else total + term
        return silu(total)

    unit = min(PAIR, length)
    per = length // unit
    i2 = lax.broadcasted_iota(jnp.int32, (unit, unit), 0)
    j2 = lax.broadcasted_iota(jnp.int32, (unit, unit), 1)
    lower = (i2 // BLOCK == j2 // BLOCK) & (i2 >= j2)
    strict = lower & (i2 > j2)

    def gates():
        lanes = gbuf.shape[2]
        total = wb_ref.shape[0]
        pick = jnp.where(
            lax.broadcasted_iota(jnp.int32, (total, lanes), 0)
            == tp * heads + lax.broadcasted_iota(jnp.int32, (total, lanes), 1), 1.0, 0.0)
        lane = lax.broadcasted_iota(jnp.int32, (1, lanes), 1)
        rate = jnp.zeros((1, lanes), f32)
        for h in range(heads):
            rate = jnp.where(lane == h, alog_ref[h], rate)
        keep = jnp.where(
            lax.broadcasted_iota(jnp.int32, (heads, lanes), 0)
            == lax.broadcasted_iota(jnp.int32, (heads, lanes), 1), 1.0, 0.0)

        def narrow(weight):
            return mm(mm(normbuf[...], weight, ((1,), (1,)), None)[halo:], pick)
        pre = narrow(wd_ref[...])
        softplus = jnp.maximum(pre, 0.0) + jnp.log1p(jnp.exp(-jnp.abs(pre)))
        log_gate = -jnp.exp(rate) * softplus + mm(extra_ref[...], keep, ((0,), (0,)))
        strength = narrow(wb_ref[...])
        row = lax.broadcasted_iota(jnp.int32, (length, length), 0)
        col = lax.broadcasted_iota(jnp.int32, (length, length), 1)
        tri = jnp.where((row // BLOCK == col // BLOCK) & (row >= col), 1.0, 0.0)
        cum = mm(tri, log_gate)
        gbuf[0] = jax.nn.sigmoid(strength)
        gbuf[1] = cum
        cum_t = cum.T
        for p in range(per):
            for h in range(heads):
                at = slice(p * unit, (p + 1) * unit)
                gaps = cum[at, h:h + 1] - cum_t[h:h + 1, at]
                sbuf[h, p] = jnp.where(lower, jnp.exp(jnp.where(lower, gaps, 0.0)), 0.0)

    all_units = [(h, p) for h in range(heads) for p in range(per)]

    def rows_of(p):
        return slice(p * unit, (p + 1) * unit)

    def keys(some):
        eye = jnp.where(i2 == j2, 1.0, 0.0)
        for h in some:
            k = unit_rows(active(1, KEY, h))
            kb = k * gbuf[0, :, h:h + 1]
            kbuf[h] = k
            for p in range(per):
                at = rows_of(p)
                corr = jnp.where(strict, mm3(halves(kb[at]), halves(k[at]), ((1,), (1,))) * sbuf[h, p], 0.0)
                ubuf[h, p] = corr
                xbuf[h, p] = eye - jnp.where(i2 // 2 == j2 // 2, corr, 0.0)
            kwbuf[h] = kb * jnp.exp(gbuf[1, :, h:h + 1])

    def level(size):
        pair = (i2 // (2 * size) == j2 // (2 * size)) & (i2 // size != j2 // size)
        done = {u: halves(xbuf[u]) for u in all_units}
        part_way = {u: mm3(halves(jnp.where(pair, ubuf[u], 0.0)), done[u]) for u in all_units}
        for u in all_units:
            xbuf[u] = xbuf[u] - mm3(done[u], halves(part_way[u]))

    def key_weights():
        for h, p in all_units:
            kwbuf[h, rows_of(p)] = mm3(halves(xbuf[h, p]), halves(kwbuf[h, rows_of(p)]))

    def queries(some):
        for h in some:
            q = unit_rows(active(0, QUERY, h)) * head_dim ** (-0.5)
            qbuf[h] = q * jnp.exp(gbuf[1, :, h:h + 1])
            for p in range(per):
                at = rows_of(p)
                sbuf[h, p] = mm3(halves(q[at]), halves(kbuf[h, at]), ((1,), (1,))) * sbuf[h, p]

    def values(some):
        for h in some:
            vb = active(2, VALUE, h) * gbuf[0, :, h:h + 1]
            for p in range(per):
                at = rows_of(p)
                fbuf[h, at] = mm3(halves(xbuf[h, p]), halves(vb[at]))

    def scan(some):
        blank = jnp.concatenate([jnp.where(
            lax.broadcasted_iota(jnp.int32, (head_dim, head_dim), 0)
            == lax.broadcasted_iota(jnp.int32, (head_dim, head_dim), 1), 1.0, 0.0),
            jnp.zeros((head_dim, head_dim), f32)], axis=1)
        for p in some:
            for b in range(unit // BLOCK):
                at = slice(p * unit + b * BLOCK, p * unit + (b + 1) * BLOCK)
                sub = slice(b * BLOCK, (b + 1) * BLOCK)
                for h in range(heads):
                    fixed = fbuf[h, at]
                    g = gbuf[1, at, h:h + 1]
                    last = g[BLOCK - 1:BLOCK]
                    fall = kbuf[h, at] * jnp.exp(last - g)
                    c = blank if p + b == 0 else cbuf[h]
                    two = mm(jnp.concatenate([kwbuf[h, at], qbuf[h, at]], axis=0), c, precision=None)
                    fresh = jnp.concatenate([jnp.zeros_like(fixed), fixed], axis=1) - two[:BLOCK]
                    pbuf[h, at, :] = two[BLOCK:] + mm(sbuf[h, p, sub, sub], fresh, precision=None)
                    cbuf[h] = jnp.exp(last) * c + mm(fall, fresh, ((0,), (0,)), None)

    def pool():
        at_row = lax.broadcasted_iota(jnp.int32, (length, group_dim), 0) + sp * length
        for i in range(groups):
            at = slice(i * group_dim, (i + 1) * group_dim)
            x = raw[POOL, :, at]
            span_of = 2 * jnp.left_shift(1, lax.rem(tp * groups + i, 4))
            total = x
            window = jnp.zeros_like(x)
            for w in (2, 4, 8, 16):
                total = total + pltpu.roll(total, w // 2, 0)
                window = window + jnp.where(span_of == w, total, 0.0)
            tally = jnp.minimum(at_row + 1, span_of).astype(f32)
            pooled = (window[halo:] / tally - x[halo:]).astype(bf16)
            mixed = jnp.dot(pooled, mix_ref[i], preferred_element_type=f32)
            pool_out[:, at] = (mixed * scale_ref[at].reshape(1, -1)).astype(bf16)

    def state_copy(h):
        return pltpu.make_async_remote_copy(
            src_ref=s_out.at[h], dst_ref=s_in.at[h], send_sem=st_s.at[h], recv_sem=st_r.at[h],
            device_id={"sp": lax.rem(sp + 1, n_sp)}, device_id_type=MESH)

    def relay():
        for h in range(heads):
            @pl.when(sp > 0)
            def _():
                state_copy(h).wait_recv()

            @pl.when(sp < n_sp - 1)
            def _():
                s_out[h] = (mm(cbuf[h, :, :head_dim], s_in[h].astype(f32), precision=None)
                            + cbuf[h, :, head_dim:]).astype(bf16)
                state_copy(h).start()

    def attend():
        for h in range(heads):
            at = slice(h * head_dim, (h + 1) * head_dim)
            attended = mm(pbuf[h, :, :head_dim], s_in[h].astype(f32), precision=None) + pbuf[h, :, head_dim:]
            scale = lax.rsqrt(jnp.mean(attended * attended, axis=-1, keepdims=True) + eps)
            delta_out[:, at] = (attended * scale * dgain_ref[...].reshape(1, -1) * silu(raw[GATE, halo:, at])).astype(bf16)

    def rs_copy(s, d, owner, dest):
        return pltpu.make_async_remote_copy(
            src_ref=part.at[s, pl.ds(pl.multiple_of(dest * rows, 16), rows)], dst_ref=rsbuf.at[s, owner],
            send_sem=rs_s.at[s, d - 1], recv_sem=rs_r.at[s, d - 1],
            device_id={"tp": lax.rem(tp + d, n_tp)}, device_id_type=MESH)

    def product(s):
        part[s] = (acc[s] + jnp.dot(delta_out[...], wbuf[OUT_DELTA, s], preferred_element_type=f32)).astype(bf16)
        for d in range(1, n_tp):
            rs_copy(s, d, tp, lax.rem(tp + d, n_tp)).start()

    def collect(s):
        total = part[s, pl.ds(pl.multiple_of(tp * rows, 16), rows)].astype(f32)
        for d in range(1, n_tp):
            owner = lax.rem(tp - d + n_tp, n_tp)
            rs_copy(s, d, owner, tp).wait_recv()
            total = total + rsbuf[s, owner].astype(f32)
        out_ref[:, pl.ds(pl.multiple_of(s * cols, cols), cols)] = total.astype(bf16)

    def pool_product(s):
        acc[s] = jnp.dot(pool_out[...], wbuf[OUT_POOL, s], preferred_element_type=f32)

    def ready(w):
        return max([gather.place(w, t) for t in range(1, n_sp)], default=0) + LAG

    turns = ready(VALUE) + 2

    def step(i):
        gather.step(i)
        if isinstance(i, int):
            for r in range(n_sp):
                if turns + 2 * r == i:
                    pl.when(sp == r)(relay)
        else:
            pl.when(i == turns + 2 * sp)(relay)

    half = (heads + 1) // 2
    middle = (per + 1) // 2
    low = halo // 16 + tp * (rows // 16)
    high = low + rows // 16
    left, right = range(half), range(half, heads)
    sizes = [2 << i for i in range((BLOCK // 2).bit_length() - 1)]

    @pl.when(sp == 0)
    def _():
        s_in[...] = jnp.zeros_like(s_in)

    def arrive_pool(t):
        gather.ready(OUT_POOL, t)
        gather.each(t, lambda src, way: pool_product(src))

    def arrive(t):
        gather.ready(OUT_DELTA, t)
        gather.each(t, lambda src, way: product(src))

    attend_at = max(turns + 2 * span, ready(POOL) + 2)
    plan = [
        (0, lambda: norm(low, high)),
        (span - 1, tokens.finish), (span - 1, lambda: norm(0, low)),
        (span, lambda: norm(high, tokbuf.shape[0] // 16)), (span, gates),
        (ready(KEY), lambda: gather.finish(KEY)), (ready(KEY), lambda: project(KEY)),
        (ready(KEY) + 1, lambda: keys(left)), (ready(KEY) + 1, lambda: keys(right)),
        (ready(QUERY), lambda: gather.finish(QUERY)), (ready(QUERY), lambda: project(QUERY)),
        (ready(QUERY) + 2, key_weights), (ready(QUERY) + 2, lambda: queries(left)),
        (ready(QUERY) + 2, lambda: gather.drain(KEY)), (ready(QUERY) + 2, lambda: queries(right)),
        (ready(VALUE), lambda: gather.finish(VALUE)), (ready(VALUE), lambda: project(VALUE)),
        (ready(VALUE), lambda: values(range(heads))), (ready(VALUE), lambda: scan(range(middle))),
        (ready(VALUE) + 1, lambda: scan(range(middle, per))), (ready(VALUE) + 1, lambda: gather.drain(QUERY)),
        (ready(GATE) + 1, lambda: gather.finish(GATE)), (ready(GATE) + 1, lambda: project(GATE)),
        (ready(GATE) + 1, lambda: gather.drain(VALUE)), (ready(GATE) + 1, tokens.drain),
        (ready(POOL), lambda: gather.finish(POOL)), (ready(POOL), lambda: project(POOL)),
        (ready(POOL) + 1, pool), (ready(POOL) + 1, lambda: gather.drain(GATE)),
        (ready(POOL) + 2, lambda: pool_product(sp)),
        (attend_at, attend), (attend_at, lambda: product(sp)), (attend_at, lambda: gather.drain(POOL)),
        (gather.end() - 1, lambda: None),
    ]
    where = [ready(KEY) + 2, ready(KEY) + 2, ready(QUERY), ready(QUERY) + 1, ready(QUERY) + 1]
    for n, size in enumerate(sizes):
        plan.append((where[min(n, len(where) - 1)], functools.partial(level, size)))
    for t in range(1, n_sp):
        pooled_at = gather.place(OUT_POOL, t) + LAG
        plan.append((max(ready(POOL) + 2, pooled_at), functools.partial(arrive_pool, t)))
        plan.append((max(attend_at, pooled_at, gather.place(OUT_DELTA, t) + LAG), functools.partial(arrive, t)))
    plan.sort(key=lambda entry: entry[0])
    reached = 0
    for at_step, act in plan:
        if at_step >= reached:
            gather.loop(reached, at_step + 1, step)
            reached = at_step + 1
        act()
    gather.drain(OUT_POOL)

    @pl.when(sp < n_sp - 1)
    def _():
        for h in range(heads):
            state_copy(h).wait_send()
    collect(sp)
    gather.loop(1, n_sp, lambda t: gather.each(t, lambda src, way: collect(src)))
    gather.drain(OUT_DELTA)

    def sent(s):
        for d in range(1, n_tp):
            rs_copy(s, d, tp, lax.rem(tp + d, n_tp)).wait_send()
    gather.loop(0, n_sp, sent)


def per_device(
    tokens,
    norm_gain,
    w_pool_in,
    w_query,
    w_key,
    w_value,
    w_gate,
    w_beta,
    w_decay,
    conv_weight,
    a_log,
    decay_extra,
    w_mix,
    pool_scale,
    delta_gain,
    w_out_pool,
    w_out_delta,
):
    n_sp, n_fs, n_tp = (lax.axis_size(a) for a in ("sp", "fs", "tp"))
    weights = (w_key, w_query, w_value, w_gate, w_pool_in, w_out_pool, w_out_delta)
    rows, width = tokens.shape
    depth, cols = w_key.shape
    heads = a_log.shape[0]
    head_dim = cols // heads
    length = n_tp * rows
    unit = min(PAIR, length)
    count = len(weights)
    lanes = 128
    slots = max(1, 2 ** max(0, len(share_bits(n_fs)) - 1) - 1)
    side = max(1, n_tp - 1)
    dma = pltpu.SemaphoreType.DMA
    vmem, anywhere = pl.BlockSpec(memory_space=pltpu.VMEM), pl.BlockSpec(memory_space=pl.ANY)
    scalars = pl.BlockSpec(memory_space=pltpu.SMEM)
    mixed = pl.pallas_call(
        functools.partial(mixer_kernel, n_sp, n_fs, n_tp),
        out_shape=pltpu.VMEM((rows, width), bf16),
        in_specs=[anywhere] + [vmem] * 4 + [scalars] + [vmem] * 4 + [anywhere] * count,
        out_specs=vmem,
        scratch_shapes=[
            pltpu.VMEM((halo + length, width), bf16),
            pltpu.VMEM((halo + length, width), bf16),
            pltpu.VMEM((count, n_sp, depth, cols), bf16),
            pltpu.VMEM((5, halo + length, cols), f32),
            pltpu.VMEM((length, cols), bf16),
            pltpu.VMEM((length, cols), bf16),
            pltpu.VMEM((heads, length, 2 * head_dim), f32),
            pltpu.VMEM((heads, head_dim, 2 * head_dim), f32),
            pltpu.VMEM((heads, head_dim, head_dim), bf16),
            pltpu.VMEM((heads, head_dim, head_dim), bf16),
            pltpu.VMEM((n_sp, length, cols), bf16),
            pltpu.VMEM((n_sp, n_tp, rows, cols), bf16),
            pltpu.VMEM((heads, length, head_dim), f32),
            pltpu.VMEM((heads, length // unit, unit, unit), f32),
            pltpu.VMEM((heads, length // unit, unit, unit), f32),
            pltpu.VMEM((heads, length, head_dim), f32),
            pltpu.VMEM((heads, length, head_dim), f32),
            pltpu.VMEM((heads, length, head_dim), f32),
            pltpu.VMEM((heads, length // unit, unit, unit), f32),
            pltpu.VMEM((2, length, lanes), f32),
            pltpu.VMEM((n_sp, length, cols), f32),
            dma((count + 1,)), dma((side,)), dma((side,)), dma((n_tp,)), dma((1,)),
            dma((count, 2)), dma((count,)), dma((count, n_sp)), dma((count,)), dma((count, n_sp, slots)),
            dma((count, n_sp)), dma((heads,)), dma((heads,)), dma((n_sp, side)), dma((n_sp, side)),
        ],
        compiler_params=pltpu.CompilerParams(collective_id=0, has_side_effects=True, vmem_limit_bytes=56 << 20),
    )(tokens, norm_gain, w_beta.T, w_decay.T, conv_weight, a_log, decay_extra.T, w_mix, pool_scale, delta_gain, *weights)

    return mixed


def solution(mesh):
    placed = (
        P(("fs", "sp", "tp"), None),
        P(),
        P("sp", "tp"),
        P("sp", "tp"),
        P("sp", "tp"),
        P("sp", "tp"),
        P("sp", "tp"),
        P(),
        P(),
        P(None, None, "tp"),
        P("tp"),
        P(("fs", "sp"), "tp"),
        P("tp", None, None),
        P("tp"),
        P(),
        P("tp", "sp"),
        P("tp", "sp"),
    )
    return jax.shard_map(
        per_device,
        mesh=mesh,
        in_specs=placed,
        out_specs=P(("fs", "sp", "tp"), None),
        check_vma=False,
    )
```

```python
import functools

import jax
import jax.numpy as jnp
from jax import lax
from jax.experimental import pallas as pl
from jax.experimental.pallas import tpu as pltpu
from jax.sharding import PartitionSpec as P

BLOCK = 64
PAIR = 2 * BLOCK

eps = 1e-06
halo = 16
MESH = pl.DeviceIdType.MESH
highest = lax.Precision.HIGHEST
f32 = jnp.float32
bf16 = jnp.bfloat16
KEY, QUERY, VALUE, GATE, POOL, OUT_POOL, OUT_DELTA = range(7)
AHEAD = 2
SKEW = 2.0
EARLY = 1.5
FINAL = 1.1
LAG = 2
UNROLL = 32


def mm(a, b, dims=((1,), (0,)), precision=highest):
    return lax.dot_general(a, b, (dims, ((), ())), precision=precision, preferred_element_type=f32)


def halves(a):
    high = a.astype(bf16)
    return high, (a - high.astype(f32)).astype(bf16)


def mm3(a, b, dims=((1,), (0,))):
    (a_high, a_low), (b_high, b_low) = a, b
    return (mm(a_high, b_high, dims, None) + mm(a_high, b_low, dims, None)) + mm(a_low, b_high, dims, None)


def rms_rows(values, gain):
    floats = values.astype(f32)
    scale = lax.rsqrt(jnp.mean(floats * floats, axis=-1, keepdims=True) + eps)
    return (floats * scale * gain.astype(f32)).astype(bf16)


def unit_rows(values):
    return values * lax.rsqrt(jnp.sum(values * values, axis=-1, keepdims=True) + eps)


def silu(x):
    return x * jax.nn.sigmoid(x)


def share_bits(n_fs):
    if n_fs & (n_fs - 1):
        return []
    return [n_fs >> (k + 1) for k in range(n_fs.bit_length() - 1)]


def both(a, b):
    if isinstance(a, bool):
        return b if a else False
    if isinstance(b, bool):
        return a if b else False
    return jnp.logical_and(a, b)


def when(cond, act):
    if isinstance(cond, bool):
        if cond:
            act()
    else:
        pl.when(cond)(act)


class Gather:
    def __init__(self, n_sp, n_fs, wbuf, z_s, z_f, z_r, f_s, f_r, last_r):
        self.n_sp, self.bits = n_sp, share_bits(n_fs)
        self.wbuf, self.z_s, self.z_f, self.z_r, self.f_s, self.f_r, self.last_r = wbuf, z_s, z_f, z_r, f_s, f_r, last_r
        self.sp, self.fs = lax.axis_index("sp"), lax.axis_index("fs")
        self.count = wbuf.shape[0]
        self.span = n_sp - 1
        self.pieces = 2 ** len(self.bits)
        self.mine = self.fs if self.bits else 0 * self.fs
        self.depth = wbuf.shape[2] // self.pieces
        self.plan_order()

    def partner(self, bit):
        return self.fs + bit * (1 - 2 * (self.fs // bit % 2))

    def mask_of(self, m, index):
        for i, bit in enumerate(self.bits):
            if m >> i & 1:
                index = index + bit * (1 - 2 * (index // bit % 2))
        return index

    def piece(self, w, src, index):
        return self.wbuf.at[w, src, pl.ds(pl.multiple_of(index * self.depth, self.depth), self.depth)]

    def z_copy(self, w, src, way, own):
        ref = self.piece(w, src, self.mine)
        to = lax.rem(self.sp + way + self.n_sp, self.n_sp)
        sent = self.z_s.at[w, (way + 1) // 2] if own else self.z_f.at[w]
        return pltpu.make_async_remote_copy(
            src_ref=ref, dst_ref=ref, send_sem=sent, recv_sem=self.z_r.at[w, src],
            device_id={"sp": to}, device_id_type=MESH)

    def f_copy(self, w, src, k, m):
        ref = self.piece(w, src, self.mask_of(m, self.mine))
        inner = k < len(self.bits) - 1
        return pltpu.make_async_remote_copy(
            src_ref=ref, dst_ref=ref, send_sem=self.f_s.at[w],
            recv_sem=self.f_r.at[w, src, 2 ** k - 1 + m] if inner else self.last_r.at[w, src],
            device_id={"fs": self.partner(self.bits[k])}, device_id_type=MESH)

    def can_send(self, way):
        return self.sp < self.n_sp - 1 if way == 1 else self.sp > 0

    def send(self, w):
        for way in (1, -1):
            @pl.when(self.can_send(way))
            def _():
                self.z_copy(w, self.sp, way, True).start()

    def each(self, t, act):
        for way in (1, -1):
            src = self.sp - way * t
            @pl.when(src >= 0 if way == 1 else src < self.n_sp)
            def _():
                act(src, way)

    def arrive_z(self, w, src, way):
        self.z_copy(w, src, way, False).wait_recv()

        @pl.when(self.can_send(way))
        def _():
            self.z_copy(w, src, way, False).start()
        for k in range(len(self.bits)):
            self.f_copy(w, src, k, 0).start()

    def arrive_f(self, w, t, k):
        def act(src, way):
            for m in range(2 ** k):
                self.f_copy(w, src, k, m).wait_recv()
                for later in range(k + 1, len(self.bits)):
                    self.f_copy(w, src, later, m | 1 << k).start()
        self.each(t, act)

    def steps(self):
        return self.count * self.span

    def plan_order(self):
        span, count = self.span, self.count
        if self.steps() > UNROLL:
            self.order, self.sends = None, None
            return
        key = {(w, t): (max(0.0, w * span - (w > 0) * EARLY - (w == count - 1) * FINAL) + SKEW * (t - 1), w) for w in range(count) for t in range(1, span + 1)}
        self.order = sorted(key, key=key.get)
        self.sends = {}
        for w in range(count):
            i = self.order.index((w, 1)) if span else 0
            while i > 0 and self.order[i - 1][1] == 1:
                i -= 1
            before = self.order[i - 1] if i > 0 else None
            at = -1 if before is None or w < AHEAD else self.order.index((before[0], before[1] - 1))
            self.sends.setdefault(at, []).append(w)

    def place(self, w, t):
        return self.order.index((w, t)) if self.order else w * self.span + t - 1

    def pair(self, i):
        if self.order:
            return self.order[min(i, len(self.order) - 1)]
        return i // self.span, i % self.span + 1

    def early(self):
        return self.sends.get(-1, []) if self.order else list(range(AHEAD))

    def step(self, i):
        if isinstance(i, int) and i < 0:
            return
        w, t = self.pair(i)
        when(i < self.steps(), lambda: self.each(t, lambda src, way: self.arrive_z(w, src, way)))
        if self.order:
            for later in self.sends.get(i, []):
                self.send(later)
        else:
            when(both(t == 1, w + AHEAD < self.count), lambda: self.send(w + AHEAD))
        for k in range(len(self.bits) - 1):
            j = i - LAG * (k + 1)

            def inner():
                w, t = self.pair(j)
                self.arrive_f(w, t, k)
            when(both(j >= 0, j < self.steps()), inner)

    def end(self):
        return self.steps() + LAG * max(0, len(self.bits) - 1)

    def ready(self, w, t):
        if self.bits:
            def act(src, way):
                ref = self.wbuf.at[w, src, pl.ds(0, self.wbuf.shape[2] // 2)]
                pltpu.make_async_copy(ref, ref, self.last_r.at[w, src]).wait()
            self.each(t, act)

    def finish(self, w):
        self.loop(1, self.n_sp, lambda t: self.ready(w, t))

    def drain(self, w):
        for way in (1, -1):
            @pl.when(self.can_send(way))
            def _():
                self.z_copy(w, self.sp, way, True).wait_send()
        if self.n_sp > 2:
            @pl.when(jnp.logical_and(self.can_send(1), self.can_send(-1)))
            def _():
                ref = self.wbuf.at[w, pl.ds(0, self.span), pl.ds(0, self.depth)]
                pltpu.make_async_copy(ref, ref, self.z_f.at[w]).wait()
        if self.bits:
            ref = self.wbuf.at[w, pl.ds(0, self.span), pl.ds(0, (self.pieces - 1) * self.depth)]
            pltpu.make_async_copy(ref, ref, self.f_s.at[w]).wait()

    def loop(self, a, b, act):
        if self.steps() <= UNROLL:
            for i in range(a, b):
                act(i)
        else:
            def body(i, c):
                act(i)
                return c
            lax.fori_loop(a, b, body, 0)


def enter(n_sp, n_fs, n_tp):
    sp, fs, tp = (lax.axis_index(a) for a in ("sp", "fs", "tp"))
    barrier = pltpu.get_barrier_semaphore()
    bits = share_bits(n_fs)

    def greet(where):
        pl.semaphore_signal(barrier, inc=1, device_id=where, device_id_type=MESH)
    right, left = sp < n_sp - 1, sp > 0
    pl.when(right)(lambda: greet({"sp": lax.rem(sp + 1, n_sp)}))
    pl.when(left)(lambda: greet({"sp": lax.rem(sp + n_sp - 1, n_sp)}))
    for bit in bits:
        greet({"fs": fs + bit * (1 - 2 * (fs // bit % 2))})
    for d in range(1, n_tp):
        greet({"tp": lax.rem(tp + d, n_tp)})
    pl.when(both(left, tp < n_tp - 1))(lambda: greet({"sp": lax.rem(sp + n_sp - 1, n_sp), "tp": n_tp - 1}))
    heard = len(bits) + n_tp - 1
    side = (n_tp - 1) * both(right, tp == n_tp - 1).astype(jnp.int32)
    pl.semaphore_wait(barrier, heard + right.astype(jnp.int32) + left.astype(jnp.int32) + side)


class Tokens:
    def __init__(self, n_sp, n_tp, tokbuf, rows, tok_s, tok_r, halo_s, halo_r):
        self.n_sp, self.n_tp, self.tokbuf, self.rows = n_sp, n_tp, tokbuf, rows
        self.tok_s, self.tok_r, self.halo_s, self.halo_r = tok_s, tok_r, halo_s, halo_r
        self.sp, self.tp = lax.axis_index("sp"), lax.axis_index("tp")
        self.end = n_tp - 1

    def tok_copy(self, d, owner):
        ref = self.tokbuf.at[pl.ds(pl.multiple_of(halo + owner * self.rows, 16), self.rows)]
        return pltpu.make_async_remote_copy(
            src_ref=ref, dst_ref=ref, send_sem=self.tok_s.at[d - 1], recv_sem=self.tok_r.at[d - 1],
            device_id={"tp": lax.rem(self.tp + d, self.n_tp)}, device_id_type=MESH)

    def halo_next(self, d):
        return pltpu.make_async_remote_copy(
            src_ref=self.tokbuf.at[pl.ds(self.n_tp * self.rows, halo)], dst_ref=self.tokbuf.at[pl.ds(0, halo)],
            send_sem=self.halo_s.at[d], recv_sem=self.halo_r.at[0],
            device_id={"sp": lax.rem(self.sp + 1, self.n_sp), "tp": lax.rem(self.tp + d, self.n_tp)},
            device_id_type=MESH)

    def start(self):
        for d in range(1, self.n_tp):
            self.tok_copy(d, self.tp).start()

    def start_halo(self):
        @pl.when(jnp.logical_and(self.tp == self.end, self.sp < self.n_sp - 1))
        def _():
            for d in range(self.n_tp):
                self.halo_next(d).start()

        @pl.when(self.sp == 0)
        def _():
            self.tokbuf[0:halo, :] = jnp.zeros((halo, self.tokbuf.shape[1]), self.tokbuf.dtype)

    def finish(self):
        for d in range(1, self.n_tp):
            self.tok_copy(d, lax.rem(self.tp - d + self.n_tp, self.n_tp)).wait_recv()

        @pl.when(self.sp > 0)
        def _():
            self.halo_next(0).wait_recv()

    def drain(self):
        for d in range(1, self.n_tp):
            self.tok_copy(d, self.tp).wait_send()

        @pl.when(jnp.logical_and(self.tp == self.end, self.sp < self.n_sp - 1))
        def _():
            for d in range(self.n_tp):
                self.halo_next(d).wait_send()


def mixer_kernel(n_sp, n_fs, n_tp, *refs):
    tok_ref, given = refs[0], refs[1:10]
    w_refs = refs[10:17]
    out_ref = refs[17]
    (tokbuf, normbuf, wbuf, raw, pool_out, delta_out, pbuf, cbuf, s_in, s_out, part, rsbuf,
     kbuf, xbuf, ubuf, kwbuf, fbuf, qbuf, sbuf, gbuf, acc,
     loc, tok_s, tok_r, halo_s, halo_r, z_s, z_f, z_r, f_s, f_r, last_r, st_s, st_r, rs_s, rs_r, small_s) = refs[18:-9]
    held = refs[-9:]
    gain_ref, wb_ref, wd_ref, conv_ref, alog_ref, extra_ref, mix_ref, scale_ref, dgain_ref = held
    small = [pltpu.make_async_copy(a, b, small_s.at[i]) for i, (a, b) in enumerate(zip(given, held))]
    rows, width = tok_ref.shape
    length = n_tp * rows
    heads, head_dim = cbuf.shape[0], cbuf.shape[1]
    groups, group_dim = mix_ref.shape[0], mix_ref.shape[1]
    sp, tp = lax.axis_index("sp"), lax.axis_index("tp")
    count = len(w_refs)
    cols = wbuf.shape[3]
    depth = wbuf.shape[2]
    local = [pltpu.make_async_copy(w_refs[i], wbuf.at[i, sp], loc.at[i]) for i in range(count)]
    here = pltpu.make_async_copy(
        tok_ref, tokbuf.at[pl.ds(pl.multiple_of(halo + tp * rows, 16), rows)], loc.at[count])
    local[0].start()
    here.start()
    for copy in local[1:] + small:
        copy.start()
    enter(n_sp, n_fs, n_tp)
    tokens = Tokens(n_sp, n_tp, tokbuf, rows, tok_s, tok_r, halo_s, halo_r)
    gather = Gather(n_sp, n_fs, wbuf, z_s, z_f, z_r, f_s, f_r, last_r)
    span = gather.span
    local[0].wait()
    gather.send(0)
    here.wait()
    tokens.start()
    for w in range(1, count):
        local[w].wait()
        if w in gather.early():
            gather.send(w)
    tokens.start_halo()
    for copy in small:
        copy.wait()

    def norm(a, b):
        def body(i, c):
            at = pl.ds(pl.multiple_of(i * 16, 16), 16)
            normbuf[at, :] = rms_rows(tokbuf[at, :], gain_ref[...].reshape(1, -1))
            return c
        lax.fori_loop(a, b, body, 0)

    def project(w):
        total = None
        for s in range(n_sp):
            term = jnp.dot(normbuf[:, s * depth:(s + 1) * depth], wbuf[w, s], preferred_element_type=f32)
            total = term if total is None else total + term
        raw[w] = total.astype(bf16).astype(f32)

    def active(role, w, h):
        at = slice(h * head_dim, (h + 1) * head_dim)
        taps = conv_ref.shape[1]
        total = None
        for j in range(taps):
            term = raw[w, pl.ds(halo - (taps - 1) + j, length), at] * conv_ref[role, j:j + 1, at]
            total = term if total is None else total + term
        return silu(total)

    unit = min(PAIR, length)
    per = length // unit
    i2 = lax.broadcasted_iota(jnp.int32, (unit, unit), 0)
    j2 = lax.broadcasted_iota(jnp.int32, (unit, unit), 1)
    lower = (i2 // BLOCK == j2 // BLOCK) & (i2 >= j2)
    strict = lower & (i2 > j2)

    def gates():
        lanes = gbuf.shape[2]
        total = wb_ref.shape[0]
        pick = jnp.where(
            lax.broadcasted_iota(jnp.int32, (total, lanes), 0)
            == tp * heads + lax.broadcasted_iota(jnp.int32, (total, lanes), 1), 1.0, 0.0)
        lane = lax.broadcasted_iota(jnp.int32, (1, lanes), 1)
        rate = jnp.zeros((1, lanes), f32)
        for h in range(heads):
            rate = jnp.where(lane == h, alog_ref[h], rate)
        keep = jnp.where(
            lax.broadcasted_iota(jnp.int32, (heads, lanes), 0)
            == lax.broadcasted_iota(jnp.int32, (heads, lanes), 1), 1.0, 0.0)

        def narrow(weight):
            return mm(mm(normbuf[...], weight, ((1,), (1,)), None)[halo:], pick)
        pre = narrow(wd_ref[...])
        softplus = jnp.maximum(pre, 0.0) + jnp.log1p(jnp.exp(-jnp.abs(pre)))
        log_gate = -jnp.exp(rate) * softplus + mm(extra_ref[...], keep, ((0,), (0,)))
        strength = narrow(wb_ref[...])
        row = lax.broadcasted_iota(jnp.int32, (length, length), 0)
        col = lax.broadcasted_iota(jnp.int32, (length, length), 1)
        tri = jnp.where((row // BLOCK == col // BLOCK) & (row >= col), 1.0, 0.0)
        cum = mm(tri, log_gate)
        gbuf[0] = jax.nn.sigmoid(strength)
        gbuf[1] = cum
        cum_t = cum.T
        for p in range(per):
            for h in range(heads):
                at = slice(p * unit, (p + 1) * unit)
                gaps = cum[at, h:h + 1] - cum_t[h:h + 1, at]
                sbuf[h, p] = jnp.where(lower, jnp.exp(jnp.where(lower, gaps, 0.0)), 0.0)

    all_units = [(h, p) for h in range(heads) for p in range(per)]

    def rows_of(p):
        return slice(p * unit, (p + 1) * unit)

    def keys(some):
        eye = jnp.where(i2 == j2, 1.0, 0.0)
        for h in some:
            k = unit_rows(active(1, KEY, h))
            kb = k * gbuf[0, :, h:h + 1]
            kbuf[h] = k
            for p in range(per):
                at = rows_of(p)
                corr = jnp.where(strict, mm3(halves(kb[at]), halves(k[at]), ((1,), (1,))) * sbuf[h, p], 0.0)
                ubuf[h, p] = corr
                xbuf[h, p] = eye - jnp.where(i2 // 2 == j2 // 2, corr, 0.0)
            kwbuf[h] = kb * jnp.exp(gbuf[1, :, h:h + 1])

    def level(size):
        pair = (i2 // (2 * size) == j2 // (2 * size)) & (i2 // size != j2 // size)
        done = {u: halves(xbuf[u]) for u in all_units}
        part_way = {u: mm3(halves(jnp.where(pair, ubuf[u], 0.0)), done[u]) for u in all_units}
        for u in all_units:
            xbuf[u] = xbuf[u] - mm3(done[u], halves(part_way[u]))

    def key_weights():
        for h, p in all_units:
            kwbuf[h, rows_of(p)] = mm3(halves(xbuf[h, p]), halves(kwbuf[h, rows_of(p)]))

    def queries(some):
        for h in some:
            q = unit_rows(active(0, QUERY, h)) * head_dim ** (-0.5)
            qbuf[h] = q * jnp.exp(gbuf[1, :, h:h + 1])
            for p in range(per):
                at = rows_of(p)
                sbuf[h, p] = mm3(halves(q[at]), halves(kbuf[h, at]), ((1,), (1,))) * sbuf[h, p]

    def values(some):
        for h in some:
            vb = active(2, VALUE, h) * gbuf[0, :, h:h + 1]
            for p in range(per):
                at = rows_of(p)
                fbuf[h, at] = mm3(halves(xbuf[h, p]), halves(vb[at]))

    def scan(some):
        blank = jnp.concatenate([jnp.where(
            lax.broadcasted_iota(jnp.int32, (head_dim, head_dim), 0)
            == lax.broadcasted_iota(jnp.int32, (head_dim, head_dim), 1), 1.0, 0.0),
            jnp.zeros((head_dim, head_dim), f32)], axis=1)
        for p in some:
            for b in range(unit // BLOCK):
                at = slice(p * unit + b * BLOCK, p * unit + (b + 1) * BLOCK)
                sub = slice(b * BLOCK, (b + 1) * BLOCK)
                for h in range(heads):
                    fixed = fbuf[h, at]
                    g = gbuf[1, at, h:h + 1]
                    last = g[BLOCK - 1:BLOCK]
                    fall = kbuf[h, at] * jnp.exp(last - g)
                    c = blank if p + b == 0 else cbuf[h]
                    two = mm(jnp.concatenate([kwbuf[h, at], qbuf[h, at]], axis=0), c, precision=None)
                    fresh = jnp.concatenate([jnp.zeros_like(fixed), fixed], axis=1) - two[:BLOCK]
                    pbuf[h, at, :] = two[BLOCK:] + mm(sbuf[h, p, sub, sub], fresh, precision=None)
                    cbuf[h] = jnp.exp(last) * c + mm(fall, fresh, ((0,), (0,)), None)

    def pool():
        at_row = lax.broadcasted_iota(jnp.int32, (length, group_dim), 0) + sp * length
        for i in range(groups):
            at = slice(i * group_dim, (i + 1) * group_dim)
            x = raw[POOL, :, at]
            span_of = 2 * jnp.left_shift(1, lax.rem(tp * groups + i, 4))
            total = x
            window = jnp.zeros_like(x)
            for w in (2, 4, 8, 16):
                total = total + pltpu.roll(total, w // 2, 0)
                window = window + jnp.where(span_of == w, total, 0.0)
            tally = jnp.minimum(at_row + 1, span_of).astype(f32)
            pooled = (window[halo:] / tally - x[halo:]).astype(bf16)
            mixed = jnp.dot(pooled, mix_ref[i], preferred_element_type=f32)
            pool_out[:, at] = (mixed * scale_ref[at].reshape(1, -1)).astype(bf16)

    def state_copy(h):
        return pltpu.make_async_remote_copy(
            src_ref=s_out.at[h], dst_ref=s_in.at[h], send_sem=st_s.at[h], recv_sem=st_r.at[h],
            device_id={"sp": lax.rem(sp + 1, n_sp)}, device_id_type=MESH)

    def relay():
        for h in range(heads):
            @pl.when(sp > 0)
            def _():
                state_copy(h).wait_recv()

            @pl.when(sp < n_sp - 1)
            def _():
                s_out[h] = (mm(cbuf[h, :, :head_dim], s_in[h].astype(f32), precision=None)
                            + cbuf[h, :, head_dim:]).astype(bf16)
                state_copy(h).start()

    def attend():
        for h in range(heads):
            at = slice(h * head_dim, (h + 1) * head_dim)
            attended = mm(pbuf[h, :, :head_dim], s_in[h].astype(f32), precision=None) + pbuf[h, :, head_dim:]
            scale = lax.rsqrt(jnp.mean(attended * attended, axis=-1, keepdims=True) + eps)
            delta_out[:, at] = (attended * scale * dgain_ref[...].reshape(1, -1) * silu(raw[GATE, halo:, at])).astype(bf16)

    def rs_copy(s, d, owner, dest):
        return pltpu.make_async_remote_copy(
            src_ref=part.at[s, pl.ds(pl.multiple_of(dest * rows, 16), rows)], dst_ref=rsbuf.at[s, owner],
            send_sem=rs_s.at[s, d - 1], recv_sem=rs_r.at[s, d - 1],
            device_id={"tp": lax.rem(tp + d, n_tp)}, device_id_type=MESH)

    def product(s):
        part[s] = (acc[s] + jnp.dot(delta_out[...], wbuf[OUT_DELTA, s], preferred_element_type=f32)).astype(bf16)
        for d in range(1, n_tp):
            rs_copy(s, d, tp, lax.rem(tp + d, n_tp)).start()

    def collect(s):
        total = part[s, pl.ds(pl.multiple_of(tp * rows, 16), rows)].astype(f32)
        for d in range(1, n_tp):
            owner = lax.rem(tp - d + n_tp, n_tp)
            rs_copy(s, d, owner, tp).wait_recv()
            total = total + rsbuf[s, owner].astype(f32)
        out_ref[:, pl.ds(pl.multiple_of(s * cols, cols), cols)] = total.astype(bf16)

    def pool_product(s):
        acc[s] = jnp.dot(pool_out[...], wbuf[OUT_POOL, s], preferred_element_type=f32)

    def ready(w):
        return max([gather.place(w, t) for t in range(1, n_sp)], default=0) + LAG

    turns = ready(VALUE) + 2

    def step(i):
        gather.step(i)
        if isinstance(i, int):
            for r in range(n_sp):
                if turns + 2 * r == i:
                    pl.when(sp == r)(relay)
        else:
            pl.when(i == turns + 2 * sp)(relay)

    half = (heads + 1) // 2
    middle = (per + 1) // 2
    low = halo // 16 + tp * (rows // 16)
    high = low + rows // 16
    left, right = range(half), range(half, heads)
    sizes = [2 << i for i in range((BLOCK // 2).bit_length() - 1)]

    @pl.when(sp == 0)
    def _():
        s_in[...] = jnp.zeros_like(s_in)

    def arrive_pool(t):
        gather.ready(OUT_POOL, t)
        gather.each(t, lambda src, way: pool_product(src))

    def arrive(t):
        gather.ready(OUT_DELTA, t)
        gather.each(t, lambda src, way: product(src))

    attend_at = max(turns + 2 * span, ready(POOL) + 2)
    plan = [
        (0, lambda: norm(low, high)),
        (span - 1, tokens.finish), (span - 1, lambda: norm(0, low)),
        (span, lambda: norm(high, tokbuf.shape[0] // 16)), (span, gates),
        (ready(KEY), lambda: gather.finish(KEY)), (ready(KEY), lambda: project(KEY)),
        (ready(KEY) + 1, lambda: keys(left)), (ready(KEY) + 1, lambda: keys(right)),
        (ready(QUERY), lambda: gather.finish(QUERY)), (ready(QUERY), lambda: project(QUERY)),
        (ready(QUERY) + 2, key_weights), (ready(QUERY) + 2, lambda: queries(left)),
        (ready(QUERY) + 2, lambda: gather.drain(KEY)), (ready(QUERY) + 2, lambda: queries(right)),
        (ready(VALUE), lambda: gather.finish(VALUE)), (ready(VALUE), lambda: project(VALUE)),
        (ready(VALUE), lambda: values(range(heads))), (ready(VALUE), lambda: scan(range(middle))),
        (ready(VALUE) + 1, lambda: scan(range(middle, per))), (ready(VALUE) + 1, lambda: gather.drain(QUERY)),
        (ready(GATE) + 1, lambda: gather.finish(GATE)), (ready(GATE) + 1, lambda: project(GATE)),
        (ready(GATE) + 1, lambda: gather.drain(VALUE)), (ready(GATE) + 1, tokens.drain),
        (ready(POOL), lambda: gather.finish(POOL)), (ready(POOL), lambda: project(POOL)),
        (ready(POOL) + 1, pool), (ready(POOL) + 1, lambda: gather.drain(GATE)),
        (ready(POOL) + 2, lambda: pool_product(sp)),
        (attend_at, attend), (attend_at, lambda: product(sp)), (attend_at, lambda: gather.drain(POOL)),
        (gather.end() - 1, lambda: None),
    ]
    where = [ready(KEY) + 2, ready(KEY) + 2, ready(QUERY), ready(QUERY) + 1, ready(QUERY) + 1]
    for n, size in enumerate(sizes):
        plan.append((where[min(n, len(where) - 1)], functools.partial(level, size)))
    for t in range(1, n_sp):
        pooled_at = gather.place(OUT_POOL, t) + LAG
        plan.append((max(ready(POOL) + 2, pooled_at), functools.partial(arrive_pool, t)))
        plan.append((max(attend_at, pooled_at, gather.place(OUT_DELTA, t) + LAG), functools.partial(arrive, t)))
    plan.sort(key=lambda entry: entry[0])
    reached = 0
    for at_step, act in plan:
        if at_step >= reached:
            gather.loop(reached, at_step + 1, step)
            reached = at_step + 1
        act()
    gather.drain(OUT_POOL)

    @pl.when(sp < n_sp - 1)
    def _():
        for h in range(heads):
            state_copy(h).wait_send()
    collect(sp)
    gather.loop(1, n_sp, lambda t: gather.each(t, lambda src, way: collect(src)))
    gather.drain(OUT_DELTA)

    def sent(s):
        for d in range(1, n_tp):
            rs_copy(s, d, tp, lax.rem(tp + d, n_tp)).wait_send()
    gather.loop(0, n_sp, sent)


def per_device(
    tokens,
    norm_gain,
    w_pool_in,
    w_query,
    w_key,
    w_value,
    w_gate,
    w_beta,
    w_decay,
    conv_weight,
    a_log,
    decay_extra,
    w_mix,
    pool_scale,
    delta_gain,
    w_out_pool,
    w_out_delta,
):
    n_sp, n_fs, n_tp = (lax.axis_size(a) for a in ("sp", "fs", "tp"))
    weights = (w_key, w_query, w_value, w_gate, w_pool_in, w_out_pool, w_out_delta)
    rows, width = tokens.shape
    depth, cols = w_key.shape
    heads = a_log.shape[0]
    head_dim = cols // heads
    length = n_tp * rows
    unit = min(PAIR, length)
    count = len(weights)
    lanes = 128
    slots = max(1, 2 ** max(0, len(share_bits(n_fs)) - 1) - 1)
    side = max(1, n_tp - 1)
    dma = pltpu.SemaphoreType.DMA
    vmem, anywhere = pl.BlockSpec(memory_space=pltpu.VMEM), pl.BlockSpec(memory_space=pl.ANY)
    small = (norm_gain, w_beta.T, w_decay.T, conv_weight, a_log, decay_extra.T, w_mix, pool_scale, delta_gain)
    held = [(pltpu.SMEM if a is a_log else pltpu.VMEM)(a.shape, a.dtype) for a in small]
    mixed = pl.pallas_call(
        functools.partial(mixer_kernel, n_sp, n_fs, n_tp),
        out_shape=pltpu.VMEM((rows, width), bf16),
        in_specs=[anywhere] * (10 + count),
        out_specs=vmem,
        scratch_shapes=[
            pltpu.VMEM((halo + length, width), bf16),
            pltpu.VMEM((halo + length, width), bf16),
            pltpu.VMEM((count, n_sp, depth, cols), bf16),
            pltpu.VMEM((5, halo + length, cols), f32),
            pltpu.VMEM((length, cols), bf16),
            pltpu.VMEM((length, cols), bf16),
            pltpu.VMEM((heads, length, 2 * head_dim), f32),
            pltpu.VMEM((heads, head_dim, 2 * head_dim), f32),
            pltpu.VMEM((heads, head_dim, head_dim), bf16),
            pltpu.VMEM((heads, head_dim, head_dim), bf16),
            pltpu.VMEM((n_sp, length, cols), bf16),
            pltpu.VMEM((n_sp, n_tp, rows, cols), bf16),
            pltpu.VMEM((heads, length, head_dim), f32),
            pltpu.VMEM((heads, length // unit, unit, unit), f32),
            pltpu.VMEM((heads, length // unit, unit, unit), f32),
            pltpu.VMEM((heads, length, head_dim), f32),
            pltpu.VMEM((heads, length, head_dim), f32),
            pltpu.VMEM((heads, length, head_dim), f32),
            pltpu.VMEM((heads, length // unit, unit, unit), f32),
            pltpu.VMEM((2, length, lanes), f32),
            pltpu.VMEM((n_sp, length, cols), f32),
            dma((count + 1,)), dma((side,)), dma((side,)), dma((n_tp,)), dma((1,)),
            dma((count, 2)), dma((count,)), dma((count, n_sp)), dma((count,)), dma((count, n_sp, slots)),
            dma((count, n_sp)), dma((heads,)), dma((heads,)), dma((n_sp, side)), dma((n_sp, side)),
            dma((9,)), *held,
        ],
        compiler_params=pltpu.CompilerParams(collective_id=0, has_side_effects=True, vmem_limit_bytes=56 << 20),
    )(tokens, *small, *weights)

    return mixed


def solution(mesh):
    placed = (
        P(("fs", "sp", "tp"), None),
        P(),
        P("sp", "tp"),
        P("sp", "tp"),
        P("sp", "tp"),
        P("sp", "tp"),
        P("sp", "tp"),
        P(),
        P(),
        P(None, None, "tp"),
        P("tp"),
        P(("fs", "sp"), "tp"),
        P("tp", None, None),
        P("tp"),
        P(),
        P("tp", "sp"),
        P("tp", "sp"),
    )
    return jax.shard_map(
        per_device,
        mesh=mesh,
        in_specs=placed,
        out_specs=P(("fs", "sp", "tp"), None),
        check_vma=False,
    )
```
